32 devices in a mesh: sp: 4 (over y, x), tp: 8 (over z, core).
Axes of the slice: x: 2, y: 2, z: 4, core: 2. Of those that a mesh axis runs over, the one named last changes fastest.
Arguments:
- stream: bfloat16 [2048, 1024], P('sp', 'tp'), may hold values from -6 to 6
- gain_first: bfloat16 [1024], P('tp'), may hold values from 0.099609375 to 1.8984375
- query_first: bfloat16 [1024, 1024], P('sp', 'tp'), may hold values from -0.1875 to 0.1875
- key_first: bfloat16 [1024, 1024], P('sp', 'tp'), may hold values from -0.1875 to 0.1875
- value_first: bfloat16 [1024, 1024], P('sp', 'tp'), may hold values from -0.1875 to 0.1875
- offset_first: float32 [8, 15, 31], P('tp'), may hold values from -4 to 254
- gain_second: bfloat16 [1024], P('tp'), may hold values from 0.099609375 to 1.8984375
- query_second: bfloat16 [1024, 1024], P('sp', 'tp'), may hold values from -0.1875 to 0.1875
- key_second: bfloat16 [1024, 1024], P('sp', 'tp'), may hold values from -0.1875 to 0.1875
- value_second: bfloat16 [1024, 1024], P('sp', 'tp'), may hold values from -0.1875 to 0.1875
- offset_second: float32 [8, 15, 31], P('tp'), may hold values from -4 to 254
Outputs:
- result: bfloat16 [2048, 1024], P('sp', 'tp')
The draws below stay inside these ranges and needn't reach their ends.
All inputs are finite; a program needn't handle non-finite values.
Results may differ from the reference program's by a relative error of at most 0.008.
Values may be sent and summed in bfloat16 or wider, within the bound.
A program may use at most 64 MiB of HBM per device.

```python
import jax
import jax.numpy as jnp
import numpy as np
from jax import lax

GRID_W = 64
HEAD_DIM = 128
HEADS = 8
D = 1024
TOKENS = 2048


def draw_stream(key, part):
    first, second = jax.random.split(jax.random.fold_in(key, 11))
    blocks = D // HEAD_DIM
    scales = jnp.exp(jax.random.uniform(first, (blocks,), jnp.float32, jnp.log(0.15), jnp.log(1.0)))
    base = jnp.clip(jax.random.normal(second, (TOKENS, D), jnp.float32), -6.0, 6.0)
    return (base * jnp.repeat(scales, HEAD_DIM)[None, :]).astype(jnp.bfloat16)


def draw_table(key):
    base = jnp.clip(jax.random.normal(key, (HEADS, 15, 31), jnp.float32), -4.0, 4.0)
    return base


def draw_offset_first(key, part):
    return draw_table(jax.random.fold_in(key, 21))


def draw_offset_second(key, part):
    return draw_table(jax.random.fold_in(key, 22))


def levels(key, dims, cuts, least, high):
    level = 1.0
    for axis_at, blocks in cuts:
        steps = jax.random.uniform(jax.random.fold_in(jax.random.fold_in(key, 6), axis_at), (blocks,), jnp.float32, least / len(cuts), high / len(cuts))
        level = level * jnp.repeat(jnp.exp(steps), dims[axis_at] // blocks).reshape((-1,) + (1,) * (len(dims) - 1 - axis_at))
    return level


def normal_values(key, shape, scale, bound, cuts=(), held_as=jnp.bfloat16):
    factor_of = levels(key, shape, cuts, -0.22, 0.18) if cuts else 1.0
    values = jax.random.normal(key, shape, jnp.float32) * scale * factor_of
    return jnp.minimum(jnp.maximum(values, -bound), bound).astype(held_as)


def setup_inputs(seed: int = 0) -> dict:
    key_of = jax.random.split(jax.random.key(seed), 12)
    stream = draw_stream(jax.random.fold_in(key_of[11], 71), 0)
    gain_first = jnp.clip(1.0 + 0.18 * jax.random.normal(key_of[1], (D,), jnp.float32), 0.099609375, 1.8984375).astype(jnp.bfloat16)
    query_first = normal_values(key_of[2], (D, D), D ** -0.5, 0.1875, ((0, 4), (1, 8)))
    key_first = normal_values(key_of[3], (D, D), D ** -0.5, 0.1875, ((0, 4), (1, 8)))
    value_first = normal_values(key_of[4], (D, D), D ** -0.5, 0.1875, ((0, 4), (1, 8)))
    offset_first = draw_offset_first(jax.random.fold_in(key_of[11], 71), 0)
    gain_second = jnp.clip(1.0 + 0.18 * jax.random.normal(key_of[6], (D,), jnp.float32), 0.099609375, 1.8984375).astype(jnp.bfloat16)
    query_second = normal_values(key_of[7], (D, D), D ** -0.5, 0.1875, ((0, 4), (1, 8)))
    key_second = normal_values(key_of[8], (D, D), D ** -0.5, 0.1875, ((0, 4), (1, 8)))
    value_second = normal_values(key_of[9], (D, D), D ** -0.5, 0.1875, ((0, 4), (1, 8)))
    offset_second = draw_offset_second(jax.random.fold_in(key_of[11], 71), 0)
    return {"stream": stream, "gain_first": gain_first, "query_first": query_first, "key_first": key_first, "value_first": value_first, "offset_first": offset_first, "gain_second": gain_second, "query_second": query_second, "key_second": key_second, "value_second": value_second, "offset_second": offset_second}


epsilon = 1e-06

def normalize(stream, gain):
    widened = stream.astype(jnp.float32)
    mean_square = lax.optimization_barrier(jnp.mean(widened * widened, axis=-1, keepdims=True))
    return (widened * lax.rsqrt(mean_square + epsilon) * gain.astype(jnp.float32)).astype(jnp.bfloat16)

def attend(query, keys, values, table, row_start, total_rows):
    rows_here, width, heads, head_size = query.shape
    blocks = width // 16
    query_cols = np.arange(width).reshape(blocks, 16)
    window_start = np.clip(query_cols - 8, 0, width - 16)
    key_cols = np.clip(np.arange(blocks) * 16 - 8, 0, width - 32)[:, None] + np.arange(32)
    column_ok = (key_cols[:, None, :] >= window_start[:, :, None]) & (key_cols[:, None, :] < window_start[:, :, None] + 16)
    column_offset = np.clip(key_cols[:, None, :] - query_cols[:, :, None] + 15, 0, 30)
    column_bias = table.astype(jnp.float32)[:, :, column_offset]
    mask = jnp.asarray(column_ok)[None, :, :, None, :]
    factor = head_size ** (-0.5)

    def one_row(index):
        grid_row = row_start + index
        first = jnp.clip(grid_row - 4, 0, total_rows - 8)
        local = first - row_start + 4
        key_block = lax.dynamic_slice_in_dim(keys, local, 8, 0)[:, key_cols].astype(jnp.float32)
        value_block = lax.dynamic_slice_in_dim(values, local, 8, 0)[:, key_cols].astype(jnp.float32)
        query_row = lax.dynamic_index_in_dim(query, index, 0, keepdims=False).reshape(blocks, 16, heads, head_size)
        scores = jnp.einsum('jqhe,mjkhe->hjqmk', query_row.astype(jnp.float32), key_block) * factor
        row_offset = first + jnp.arange(8, dtype=jnp.int32) - grid_row + 7
        row_bias = jnp.transpose(jnp.take(column_bias, row_offset, axis=1), (0, 2, 3, 1, 4))
        scores = jnp.where(mask, scores + row_bias, -1e+30)
        weight = jax.nn.softmax(scores.reshape(heads, blocks, 16, 256), axis=-1)
        rounded = weight.astype(jnp.bfloat16).reshape(heads, blocks, 16, 8, 32)
        output = jnp.einsum('hjqmk,mjkhe->jqhe', rounded.astype(jnp.float32), value_block)
        return output.reshape(width, heads * head_size)
    return lax.map(one_row, jnp.arange(rows_here, dtype=jnp.int32))

def layer(stream, gain, w_query, w_key, w_value, table):
    normed = normalize(stream, gain)
    query = jnp.dot(normed, w_query, preferred_element_type=jnp.float32).astype(jnp.bfloat16)
    keys = jnp.dot(normed, w_key, preferred_element_type=jnp.float32).astype(jnp.bfloat16)
    values = jnp.dot(normed, w_value, preferred_element_type=jnp.float32).astype(jnp.bfloat16)
    total_rows = stream.shape[0] // GRID_W
    shape = (total_rows, GRID_W, HEADS, HEAD_DIM)
    padding = ((4, 4), (0, 0), (0, 0), (0, 0))
    keys = jnp.pad(keys.reshape(shape), padding)
    values = jnp.pad(values.reshape(shape), padding)
    output = attend(query.reshape(shape), keys, values, table, 0, total_rows)
    return (stream.astype(jnp.float32) + output.reshape(stream.shape)).astype(jnp.bfloat16)

def reference(stream, gain_first, query_first, key_first, value_first, offset_first, gain_second, query_second, key_second, value_second, offset_second):
    middle = layer(stream, gain_first, query_first, key_first, value_first, offset_first)
    return layer(middle, gain_second, query_second, key_second, value_second, offset_second)
```

```python
import functools

import jax
import jax.numpy as jnp
from jax import lax
from jax.experimental import pallas as pl
from jax.experimental.pallas import tpu as pltpu
from jax.sharding import PartitionSpec as P

GRID_W = 64
WIN_R = 8
WIN_C = 16
HALO = 4
GAIN_ROWS = 16
LAG = 2
BATCH = (4, 4)
QUERY_AT = (3, 0)
W_AFTER = 0
epsilon = 1e-06
MESH = pl.DeviceIdType.MESH


def build_bias(table_ref, rows_ref, tiles_ref):
    rows_ref[...] = jnp.zeros_like(rows_ref)
    rows_ref[0 : 2 * WIN_R - 1, 0 : 2 * WIN_C - 1] = table_ref[:, 0, :]
    shape = (GRID_W, 2 * GRID_W)
    column = lax.broadcasted_iota(jnp.int32, shape, 0)
    key_column = lax.broadcasted_iota(jnp.int32, shape, 1)
    key_column = jnp.where(key_column >= GRID_W, key_column - GRID_W, key_column)
    start = jnp.clip(column - WIN_C // 2, 0, GRID_W - WIN_C)
    inside = (key_column >= start) & (key_column < start + WIN_C)
    for o in range(2 * WIN_R - 2):
        pair = rows_ref[o : o + 1, :] + pltpu.roll(rows_ref[o + 1 : o + 2, :], GRID_W, 1)
        tile = pltpu.roll(
            jnp.broadcast_to(pair, shape), 2 * GRID_W - (WIN_C - 1), 1, stride=1, stride_axis=0
        )
        tiles_ref[o] = jnp.where(inside, tile, -1e30)


def row_orders(rows_dev):
    last = rows_dev - HALO - 1 if rows_dev >= WIN_R else -1
    high = [(r, min(2, rows_dev - r)) for r in range(rows_dev - HALO, rows_dev, 2)]
    low = [(r, min(2, last - r)) for r in range(0, last, 2)]
    if last < 0:
        low = [(r, min(2, rows_dev - HALO - r)) for r in range(0, rows_dev - HALO, 2)]
        return (low + high, high + low)
    return (low + high + [(last, 1)], high + low + [(last, 1)])


def kernel(
    n_sp,
    n_tp,
    x_ref,
    gain_a,
    gain_b,
    wq_a,
    wk_a,
    wv_a,
    wq_b,
    wk_b,
    wv_b,
    table_a,
    table_b,
    out_ref,
    xg_a,
    xg_b,
    wkv_a,
    wkv_b,
    wqg_a,
    wqg_b,
    kvp_a,
    kvp_b,
    q_buf,
    normed,
    rows_buf,
    tiles_a,
    tiles_b,
    load_sem,
    xs_sem,
    xr_sem,
    xp_sem,
    ws_sem,
    wr_sem,
    hs_sem,
    hr_sem,
):
    sp = lax.axis_index("sp")
    tp = lax.axis_index("tp")
    tokens, feat = x_ref.shape
    depth = wq_a.shape[0]
    rows_dev = tokens // GRID_W
    total_rows = rows_dev * n_sp
    half = n_tp // 2
    core = lax.rem(tp, 2)
    z = tp // 2
    partner = tp + 1 - 2 * core
    low = HALO * GRID_W
    below_rows = HALO - 1 if rows_dev >= WIN_R else HALO
    below = below_rows * GRID_W
    factor = feat ** (-0.5)
    orders = row_orders(rows_dev)
    chunks = len(orders[0])

    xg = (xg_a, xg_b)
    wkv = (wkv_a, wkv_b)
    wqg = (wqg_a, wqg_b)
    kvp = (kvp_a, kvp_b)
    tiles = (tiles_a, tiles_b)

    sp_peers = [lax.rem(sp + k, n_sp) for k in range(1, n_sp)]
    has_next = sp < n_sp - 1
    has_previous = sp > 0
    has_right = z < half - 1
    has_left = z > 0

    barrier = pltpu.get_barrier_semaphore()

    def greet(s, t):
        pl.semaphore_signal(barrier, inc=1, device_id=(s, t), device_id_type=MESH)

    pl.when(has_right)(lambda: greet(sp, tp + 2))
    pl.when(has_left)(lambda: greet(sp, tp - 2))
    for s in sp_peers:
        greet(s, tp)
    greet(sp, partner)

    def slot_of(c, j):
        return c * half + j

    own = slot_of(core, z)

    def w_rows(device):
        return pl.ds(pl.multiple_of(device * depth, depth), depth)

    mine = w_rows(sp)

    def place(layer, row):
        at = GAIN_ROWS if layer == 0 else 0
        for first, size in orders[layer]:
            if first <= row < first + size:
                return at + (row - first) * GRID_W
            at += size * GRID_W

    def span(layer, c):
        first, size = orders[layer][c]
        at, size = place(layer, first), size * GRID_W
        if layer == 0 and c == 0:
            return pl.ds(0, size + GAIN_ROWS)
        return pl.ds(at, size)

    runs = []
    for first, size in orders[0]:
        if runs and sum(runs[-1]) == first:
            runs[-1] = (runs[-1][0], runs[-1][1] + size)
        else:
            runs.append((first, size))
    for first, size in runs:
        pltpu.make_async_copy(
            x_ref.at[pl.ds(first * GRID_W, size * GRID_W)],
            xg_a.at[own, pl.ds(place(0, first), size * GRID_W)],
            load_sem.at[0],
        ).start()
    loads = (
        (1, wk_a, wkv_a.at[mine, pl.ds(0, feat)]),
        (1, wv_a, wkv_a.at[mine, pl.ds(feat, feat)]),
        (2, wq_a, wqg_a.at[mine]),
        (3, wk_b, wkv_b.at[mine, pl.ds(0, feat)]),
        (3, wv_b, wkv_b.at[mine, pl.ds(feat, feat)]),
        (4, wq_b, wqg_b.at[mine]),
    )
    for i, src, dst in loads:
        pltpu.make_async_copy(src, dst, load_sem.at[i]).start()

    def loaded(i, ref):
        pltpu.make_async_copy(ref, ref, load_sem.at[i]).wait()

    spare = jnp.zeros((GAIN_ROWS - 2, feat), jnp.float32)
    both = [gain_a[...].astype(jnp.float32), gain_b[...].astype(jnp.float32), spare]
    xg_a[own, 0:GAIN_ROWS, :] = jnp.concatenate(both, axis=0).astype(jnp.bfloat16)

    def remote(src, dst, send, recv, device):
        return pltpu.make_async_remote_copy(
            src_ref=src,
            dst_ref=dst,
            send_sem=send,
            recv_sem=recv,
            device_id=device,
            device_id_type=MESH,
        )

    def x_copy(layer, c, j, target):
        ref = xg[layer].at[slot_of(core, j), span(layer, c)]
        index = lax.rem(j - target + half, half) - 1
        device = (sp, 2 * target + core)
        return remote(ref, ref, xs_sem.at[layer], xr_sem.at[layer, c, index], device)

    def x_pass(layer, c, j):
        ref = xg[layer].at[slot_of(core, j), span(layer, c)]
        return remote(ref, ref, xs_sem.at[layer], xp_sem.at[layer, c], (sp, partner))

    def x_start(layer, c):
        pl.when(has_right)(lambda: x_copy(layer, c, z, z + 1).start())
        pl.when(has_left)(lambda: x_copy(layer, c, z, z - 1).start())
        x_pass(layer, c, z).start()

    both_sides = jnp.minimum(z, half - 1 - z)
    far = jnp.where(2 * z < half, 1, -1)

    def source(k):
        paired = k <= 2 * both_sides
        away = jnp.where(paired, (k + 1) // 2, k - both_sides)
        side = jnp.where(paired, 1 if k % 2 else -1, far)
        return z + away * side, side

    sources = [source(k) for k in range(1, half)]

    def x_take(layer, c, k):
        j, side = sources[k - 1]
        index = lax.rem(j - z + half, half) - 1
        ref = xg[layer].at[slot_of(core, j), span(layer, c)]
        remote(ref, ref, xs_sem.at[layer], xr_sem.at[layer, c, index], (sp, partner)).wait_recv()
        onward = jnp.where(side > 0, has_left, has_right)
        pl.when(onward)(lambda: x_copy(layer, c, j, z - side).start())
        x_pass(layer, c, j).start()

    def x_finish(layer, c):
        ref = xg[layer].at[pl.ds((1 - core) * half, half), span(layer, c)]
        remote(ref, ref, xs_sem.at[layer], xp_sem.at[layer, c], (sp, partner)).wait_recv()

    def x_sent(layer, counts):
        for count in counts:
            ref = xg[layer].at[pl.ds(0, count)]
            remote(ref, ref, xs_sem.at[layer], xp_sem.at[layer, 0], (sp, partner)).wait_send()

    def x_drain(layer):
        for at in range(half):
            count = half
            count += at + 1 if at < half - 1 else 0
            count += half - at if at > 0 else 0
            counts = [n_tp] * (count // n_tp) + [count % n_tp] * (count % n_tp > 0)
            pl.when(z == at)(functools.partial(x_sent, layer, counts))

    def w_copy(layer, which, slot, target):
        ref = (wkv, wqg)[which][layer].at[w_rows(slot)]
        return remote(ref, ref, ws_sem.at[layer, which], wr_sem.at[layer, which], (target, tp))

    def w_start(layer, which):
        for target in sp_peers:
            w_copy(layer, which, sp, target).start()

    def w_all(layer, which):
        ref = (wkv, wqg)[which][layer].at[pl.ds(0, (n_sp - 1) * depth)]
        return remote(ref, ref, ws_sem.at[layer, which], wr_sem.at[layer, which], (sp, partner))

    def halo(layer, way, src, dst, size):
        buf = kvp[layer]
        target = lax.rem(sp + 1, n_sp) if way == 0 else lax.rem(sp + n_sp - 1, n_sp)
        return remote(
            buf.at[pl.ds(src, size)],
            buf.at[pl.ds(dst, size)],
            hs_sem.at[layer, way],
            hr_sem.at[layer, way],
            (target, tp),
        )

    def halo_start(layer, first, size):
        start = max(first, rows_dev - HALO)
        if start < first + size:
            src = low + start * GRID_W
            rows = (first + size - start) * GRID_W
            pl.when(has_next)(lambda: halo(layer, 0, src, src - tokens, rows).start())
        stop = min(first + size, below_rows)
        if first < stop:
            src = low + first * GRID_W
            rows = (stop - first) * GRID_W
            pl.when(has_previous)(lambda: halo(layer, 1, src, src + tokens, rows).start())

    def halo_all(layer, way):
        at, size = ((0, low), (low + tokens, below))[way]
        return halo(layer, way, at, at, size)

    def norm(layer, c):
        buf = xg[layer]
        first, size = orders[layer][c]
        for row in range(first, first + size):
            at = pl.ds(place(layer, row), GRID_W)
            to = pl.ds(row * GRID_W, GRID_W)
            total = jnp.zeros((GRID_W, feat), jnp.float32)
            for s in range(n_tp):
                wide = buf[s, at, :].astype(jnp.float32)
                total = total + wide * wide
            mean = jnp.sum(total, axis=-1, keepdims=True) * (1.0 / (n_tp * feat))
            scale = lax.rsqrt(mean + epsilon)
            for s in range(n_tp):
                slot = slot_of(s % 2, s // 2)
                gain = xg_a[slot, 0:GAIN_ROWS, :][layer : layer + 1, :]
                wide = buf[slot, at, :].astype(jnp.float32)
                normed[to, s * feat : (s + 1) * feat] = (
                    wide * scale * gain.astype(jnp.float32)
                ).astype(jnp.bfloat16)

    def project(weights, dst, offset, first, size):
        at, rows = first * GRID_W, size * GRID_W
        made = jnp.dot(
            normed[at : at + rows, :], weights[...], preferred_element_type=jnp.float32
        )
        dst[pl.ds(offset + at, rows), :] = made.astype(jnp.bfloat16)

    def attend(layer, indices):
        places, scores = [], []
        for index in indices:
            row = sp * rows_dev + index
            first = jnp.minimum(jnp.maximum(row - HALO, 0), total_rows - WIN_R)
            local = first - sp * rows_dev + HALO
            base = first - row + WIN_R - 1
            at = pl.ds(pl.multiple_of(local * GRID_W, GRID_W), WIN_R * GRID_W)
            query = q_buf[index * GRID_W : (index + 1) * GRID_W, :]
            raw = lax.dot_general(
                query,
                kvp[layer][at, 0:feat],
                (((1,), (1,)), ((), ())),
                preferred_element_type=jnp.float32,
            )
            bias = jnp.concatenate([tiles[layer][base + 2 * j] for j in range(WIN_R // 2)], axis=1)
            places.append(at)
            scores.append(raw * factor + bias)
        tops = [jnp.max(score, axis=-1, keepdims=True) for score in scores]
        weights = [jnp.exp(score - top) for score, top in zip(scores, tops)]
        scales = [1.0 / jnp.sum(weight, axis=-1, keepdims=True) for weight in weights]
        outs = [
            jnp.dot(
                (weight * scale).astype(jnp.bfloat16),
                kvp[layer][at, feat : 2 * feat],
                preferred_element_type=jnp.float32,
            )
            for weight, scale, at in zip(weights, scales, places)
        ]
        made = []
        for index, out in zip(indices, outs):
            wide = xg[layer][own, pl.ds(place(layer, index), GRID_W), :].astype(jnp.float32)
            made.append((wide + out).astype(jnp.bfloat16))
        return made

    sync = 1 + (n_sp - 1) + has_right.astype(jnp.int32) + has_left.astype(jnp.int32)
    pl.semaphore_wait(barrier, sync)
    loaded(0, xg_a.at[own, pl.ds(GAIN_ROWS, tokens)])
    for c in range(chunks):
        x_start(0, c)
    loaded(1, wkv_a.at[mine])
    w_start(0, 0)
    loaded(2, wqg_a.at[mine])
    w_start(0, 1)
    build_bias(table_a, rows_buf, tiles_a)
    build_bias(table_b, rows_buf, tiles_b)
    loaded(3, wkv_b.at[mine])
    loaded(4, wqg_b.at[mine])

    high_rows = list(range(rows_dev - HALO, rows_dev))
    low_rows = [i for i in range(rows_dev) if i not in high_rows]
    for layer in range(2):
        last = half - 1
        early = [(k, k + 1) for k in range(1, last - 1, 2)]
        rest = list(range(2 * len(early) + 1, last))
        for group in early + [(k,) for k in rest]:
            for c in range(chunks):
                for k in group:
                    x_take(layer, c, k)
        ready = QUERY_AT[layer]
        for c in range(chunks + LAG):
            if c < chunks:
                x_take(layer, c, last)
            if c < LAG:
                continue
            x_finish(layer, c - LAG)
            norm(layer, c - LAG)
            if c == LAG:
                w_all(layer, 0).wait_recv()
            first, size = orders[layer][c - LAG]
            project(wkv[layer], kvp[layer], low, first, size)
            halo_start(layer, first, size)
            if c - LAG == min(ready, chunks - 1):
                w_all(layer, 1).wait_recv()
                for part in orders[layer][: c - LAG + 1]:
                    project(wqg[layer], q_buf, 0, *part)
            elif c - LAG > ready:
                project(wqg[layer], q_buf, 0, first, size)

        groups = ((1, high_rows), (0, low_rows)) if layer == 0 else ((0, low_rows), (1, high_rows))
        if rows_dev < WIN_R:
            groups = ((0, []), (1, high_rows), (0, low_rows))
        waited, finished, sent = set(), set(), 0
        for way, rows in groups:
            if way not in waited:
                waited.add(way)
                pl.when((has_next, has_previous)[1 - way])(halo_all(layer, way).wait_recv)
            for at in range(0, len(rows), BATCH[layer]):
                batch = rows[at : at + BATCH[layer]]
                for index, made in zip(batch, attend(layer, batch)):
                    if layer == 1:
                        out_ref[index * GRID_W : (index + 1) * GRID_W, :] = made
                    else:
                        xg_b[own, pl.ds(place(1, index), GRID_W), :] = made
                        finished.add(index)
                while layer == 0 and sent < chunks:
                    first, size = orders[1][sent]
                    if not set(range(first, first + size)) <= finished:
                        break
                    x_start(1, sent)
                    sent += 1
            if layer == 0 and way == W_AFTER:
                w_start(1, 0)
                w_start(1, 1)

    for layer in range(2):
        pl.when(has_next)(halo_all(layer, 0).wait_send)
        pl.when(has_previous)(halo_all(layer, 1).wait_send)
        w_all(layer, 0).wait_send()
        w_all(layer, 1).wait_send()
        x_drain(layer)


def body(n_sp, n_tp, stream, gain_a, wq_a, wk_a, wv_a, table_a, gain_b, wq_b, wk_b, wv_b, table_b):
    tokens, feat = stream.shape
    depth = wq_a.shape[0] * n_sp
    rows_dev = tokens // GRID_W
    chunks = len(row_orders(rows_dev)[0])
    bf16 = jnp.bfloat16
    padded = tokens + 2 * HALO * GRID_W
    hbm = pl.BlockSpec(memory_space=pl.ANY)
    vmem = pl.BlockSpec(memory_space=pltpu.VMEM)
    dma = pltpu.SemaphoreType.DMA
    return pl.pallas_call(
        functools.partial(kernel, n_sp, n_tp),
        out_shape=pltpu.VMEM((tokens, feat), bf16),
        in_specs=[hbm] + [vmem] * 2 + [hbm] * 6 + [vmem] * 2,
        out_specs=vmem,
        scratch_shapes=[
            pltpu.VMEM((n_tp, tokens + GAIN_ROWS, feat), bf16),
            pltpu.VMEM((n_tp, tokens, feat), bf16),
            pltpu.VMEM((depth, 2 * feat), bf16),
            pltpu.VMEM((depth, 2 * feat), bf16),
            pltpu.VMEM((depth, feat), bf16),
            pltpu.VMEM((depth, feat), bf16),
            pltpu.VMEM((padded, 2 * feat), bf16),
            pltpu.VMEM((padded, 2 * feat), bf16),
            pltpu.VMEM((tokens, feat), bf16),
            pltpu.VMEM((tokens, n_tp * feat), bf16),
            pltpu.VMEM((2 * WIN_R, 2 * GRID_W), jnp.float32),
            pltpu.VMEM((2 * WIN_R - 2, GRID_W, 2 * GRID_W), jnp.float32),
            pltpu.VMEM((2 * WIN_R - 2, GRID_W, 2 * GRID_W), jnp.float32),
            dma((5,)),
            dma((2,)),
            dma((2, chunks, n_tp // 2 - 1)),
            dma((2, chunks)),
            dma((2, 2)),
            dma((2, 2)),
            dma((2, 2)),
            dma((2, 2)),
        ],
        compiler_params=pltpu.CompilerParams(collective_id=0, has_side_effects=True),
    )(
        stream,
        gain_a.reshape(1, feat),
        gain_b.reshape(1, feat),
        wq_a,
        wk_a,
        wv_a,
        wq_b,
        wk_b,
        wv_b,
        jnp.transpose(table_a, (1, 0, 2)),
        jnp.transpose(table_b, (1, 0, 2)),
    )


def solution(mesh):
    placed = (
        P("sp", "tp"),
        P("tp"),
        P("sp", "tp"),
        P("sp", "tp"),
        P("sp", "tp"),
        P("tp", None, None),
        P("tp"),
        P("sp", "tp"),
        P("sp", "tp"),
        P("sp", "tp"),
        P("tp", None, None),
    )
    return jax.shard_map(
        functools.partial(body, mesh.shape["sp"], mesh.shape["tp"]),
        mesh=mesh,
        in_specs=placed,
        out_specs=P("sp", "tp"),
        check_vma=False,
    )
```

```python
import functools

import jax
import jax.numpy as jnp
from jax import lax
from jax.experimental import pallas as pl
from jax.experimental.pallas import tpu as pltpu
from jax.sharding import PartitionSpec as P

GRID_W = 64
WIN_R = 8
WIN_C = 16
HALO = 4
GAIN_ROWS = 16
LAG = (1, 1)
DIRECT = (0, 4)
DEFER = ((0, 0, 0, 0), (1, 2, 3, 0))
BATCH = 4
W_STEP = 2
epsilon = 1e-06
MESH = pl.DeviceIdType.MESH


def build_bias(table_ref, rows_ref, tiles_ref):
    rows_ref[...] = jnp.zeros_like(rows_ref)
    rows_ref[0 : 2 * WIN_R - 1, 0 : 2 * WIN_C - 1] = table_ref[:, 0, :]
    shape = (GRID_W, 2 * GRID_W)
    column = lax.broadcasted_iota(jnp.int32, shape, 0)
    key_column = lax.broadcasted_iota(jnp.int32, shape, 1)
    key_column = jnp.where(key_column >= GRID_W, key_column - GRID_W, key_column)
    start = jnp.clip(column - WIN_C // 2, 0, GRID_W - WIN_C)
    inside = (key_column >= start) & (key_column < start + WIN_C)
    for o in range(2 * WIN_R - 2):
        pair = rows_ref[o : o + 1, :] + pltpu.roll(rows_ref[o + 1 : o + 2, :], GRID_W, 1)
        tile = pltpu.roll(
            jnp.broadcast_to(pair, shape), 2 * GRID_W - (WIN_C - 1), 1, stride=1, stride_axis=0
        )
        tiles_ref[o] = jnp.where(inside, tile, -1e30)


def row_orders(rows_dev):
    if rows_dev < WIN_R:
        each = [[r] for r in range(rows_dev)]
        return (each, each)
    edge, last = rows_dev - HALO, rows_dev - 1
    inner = list(range(HALO - 1, edge))
    first = [[0, last], [1, last - 1], [2, last - 2], inner + [edge]]
    second = [inner + [edge, edge + 1], [2, last - 1], [1, last], [0]]
    return (first, second)


def halo_plan(rows_dev, layer):
    below = HALO - 1 if rows_dev >= WIN_R else HALO
    edge, plan = rows_dev - HALO, []
    for chunk in row_orders(rows_dev)[layer]:
        up = [(1, row) for row in chunk if row < below]
        plan.append(up + [(0, row) for row in chunk if row >= edge])
    if rows_dev < WIN_R:
        return plan
    late = DEFER[layer]
    held = []
    for c, sends in enumerate(plan):
        ups = [send for send in sends if send[0] == 1]
        downs = held + [send for send in sends if send[0] == 0]
        held = downs[max(len(downs) - late[c], 0) :]
        plan[c] = ups + downs[: max(len(downs) - late[c], 0)]
    return plan


def row_groups(rows_dev, layer):
    every = list(range(rows_dev))
    below = HALO - 1 if rows_dev >= WIN_R else HALO
    edge, last = rows_dev - HALO, rows_dev - 1
    up = [(1, r) for r in range(below)]
    down = [(0, r) for r in range(edge, rows_dev)]
    if rows_dev < WIN_R:
        return [(up + down, every)]
    if layer == 0:
        return [
            ([(1, 0), (0, last)], every[3 : edge + 2]),
            ([(1, 1), (0, last - 1)], [2, last - 1]),
            ([(1, 2), (0, last - 2)], [1, last]),
            ([(0, edge)], [0]),
        ]
    return [(up, every[edge:]), (down, every[:edge])]


def kernel(
    n_sp,
    n_tp,
    x_ref,
    gain_a,
    gain_b,
    wq_a,
    wk_a,
    wv_a,
    wq_b,
    wk_b,
    wv_b,
    table_a,
    table_b,
    out_ref,
    xg_a,
    xg_b,
    w_a,
    w_b,
    kvp_a,
    kvp_b,
    q_buf,
    normed,
    gains_buf,
    tables_buf,
    rows_buf,
    tiles_a,
    tiles_b,
    load_sem,
    xs_sem,
    xr_sem,
    xp_sem,
    ws_sem,
    wr_sem,
    hs_sem,
    hr_sem,
):
    sp = lax.axis_index("sp")
    tp = lax.axis_index("tp")
    tokens, feat = x_ref.shape
    depth = wq_a.shape[0]
    rows_dev = tokens // GRID_W
    total_rows = rows_dev * n_sp
    half = n_tp // 2
    core = lax.rem(tp, 2)
    z = tp // 2
    partner = tp + 1 - 2 * core
    low = HALO * GRID_W
    below_rows = HALO - 1 if rows_dev >= WIN_R else HALO
    below = below_rows * GRID_W
    factor = feat ** (-0.5)
    orders = row_orders(rows_dev)
    chunks = len(orders[0])

    xg = (xg_a, xg_b)
    w = (w_a, w_b)
    kvp = (kvp_a, kvp_b)
    tiles = (tiles_a, tiles_b)

    square = n_sp == 4
    near_x = sp + 1 - 2 * lax.rem(sp, 2)
    near_y = lax.rem(sp + 2, n_sp)
    sp_peers = [lax.rem(sp + k, n_sp) for k in range(1, n_sp)]
    has_next = sp < n_sp - 1
    has_previous = sp > 0
    has_right = z < half - 1
    has_left = z > 0
    is_end = jnp.logical_not(has_left & has_right)
    crossed = (sp == 1) | (sp == 2)

    barrier = pltpu.get_barrier_semaphore()

    def greet(s, t):
        pl.semaphore_signal(barrier, inc=1, device_id=(s, t), device_id_type=MESH)

    pl.when(has_right)(lambda: greet(sp, tp + 2))
    pl.when(has_left)(lambda: greet(sp, tp - 2))
    for s in (near_x, near_y) if square else sp_peers:
        greet(s, tp)
    if square:
        pl.when(crossed)(lambda: greet(3 - sp, tp))
    greet(sp, partner)

    def slot_of(c, j):
        return c * half + j

    own = slot_of(core, z)

    def w_rows(device):
        return pl.ds(pl.multiple_of(device * depth, depth), depth)

    mine = w_rows(sp)

    flat = [[row for chunk in order for row in chunk] for order in orders]

    def place(layer, row):
        return flat[layer].index(row) * GRID_W + (GAIN_ROWS if layer == 0 else 0)

    def span(layer, c):
        at, size = place(layer, orders[layer][c][0]), len(orders[layer][c]) * GRID_W
        if layer == 0 and c == 0:
            return pl.ds(0, size + GAIN_ROWS)
        return pl.ds(at, size)

    runs = []
    for row in flat[0]:
        if runs and runs[-1][-1] == row - 1:
            runs[-1].append(row)
        else:
            runs.append([row])
    for run in runs:
        pltpu.make_async_copy(
            x_ref.at[pl.ds(run[0] * GRID_W, len(run) * GRID_W)],
            xg_a.at[own, pl.ds(place(0, run[0]), len(run) * GRID_W)],
            load_sem.at[0],
        ).start()
    loads = [
        (1, wk_a, w_a.at[mine, pl.ds(0, feat)]),
        (1, wv_a, w_a.at[mine, pl.ds(feat, feat)]),
        (1, wq_a, w_a.at[mine, pl.ds(2 * feat, feat)]),
        (3, gain_a, gains_buf.at[0]),
        (4, gain_b, gains_buf.at[1]),
        (5, table_a, tables_buf.at[0]),
        (6, table_b, tables_buf.at[1]),
        (2, wk_b, w_b.at[mine, pl.ds(0, feat)]),
        (2, wv_b, w_b.at[mine, pl.ds(feat, feat)]),
        (2, wq_b, w_b.at[mine, pl.ds(2 * feat, feat)]),
    ]
    for i, src, dst in loads:
        pltpu.make_async_copy(src, dst, load_sem.at[i]).start()

    def loaded(i, ref):
        pltpu.make_async_copy(ref, ref, load_sem.at[i]).wait()

    loaded(3, gains_buf.at[0])
    loaded(4, gains_buf.at[1])
    spare = jnp.zeros((GAIN_ROWS - 2, feat), jnp.float32)
    both = [gains_buf[0].astype(jnp.float32), gains_buf[1].astype(jnp.float32), spare]
    xg_a[own, 0:GAIN_ROWS, :] = jnp.concatenate(both, axis=0).astype(jnp.bfloat16)

    def remote(src, dst, send, recv, device):
        return pltpu.make_async_remote_copy(
            src_ref=src,
            dst_ref=dst,
            send_sem=send,
            recv_sem=recv,
            device_id=device,
            device_id_type=MESH,
        )

    def x_copy(layer, c, j, target):
        ref = xg[layer].at[slot_of(core, j), span(layer, c)]
        index = lax.rem(j - target + half, half) - 1
        device = (sp, 2 * target + core)
        return remote(ref, ref, xs_sem.at[layer], xr_sem.at[layer, c, index], device)

    def x_pass(layer, c, j):
        ref = xg[layer].at[slot_of(core, j), span(layer, c)]
        return remote(ref, ref, xs_sem.at[layer], xp_sem.at[layer, c], (sp, partner))

    def x_start(layer, c):
        for far in (2, 1)[c >= DIRECT[layer] :]:
            pl.when(z + far < half)(lambda far=far: x_copy(layer, c, z, z + far).start())
            pl.when(z - far >= 0)(lambda far=far: x_copy(layer, c, z, z - far).start())
        x_pass(layer, c, z).start()

    both_sides = jnp.minimum(z, half - 1 - z)
    far = jnp.where(2 * z < half, 1, -1)

    def source(k):
        paired = k <= 2 * both_sides
        away = jnp.where(paired, (k + 1) // 2, k - both_sides)
        side = jnp.where(paired, 1 if k % 2 else -1, far)
        return z + away * side, side, away

    sources = [source(k) for k in range(1, half)]

    def x_take(layer, c, k):
        j, side, away = sources[k - 1]
        index = lax.rem(j - z + half, half) - 1
        ref = xg[layer].at[slot_of(core, j), span(layer, c)]
        remote(ref, ref, xs_sem.at[layer], xr_sem.at[layer, c, index], (sp, partner)).wait_recv()
        onward = jnp.where(side > 0, has_left, has_right)
        if c < DIRECT[layer]:
            onward &= away >= 2
        pl.when(onward)(lambda: x_copy(layer, c, j, z - side).start())
        x_pass(layer, c, j).start()

    def x_finish(layer, c):
        ref = xg[layer].at[pl.ds((1 - core) * half, half), span(layer, c)]
        remote(ref, ref, xs_sem.at[layer], xp_sem.at[layer, c], (sp, partner)).wait_recv()

    def x_sent(layer, counts):
        for c, count in enumerate(counts):
            for part in [n_tp] * (count // n_tp) + [count % n_tp] * (count % n_tp > 0):
                ref = xg[layer].at[pl.ds(0, part), span(layer, c)]
                sems = xs_sem.at[layer], xp_sem.at[layer, 0]
                remote(ref, ref, *sems, (sp, partner)).wait_send()

    def x_drain(layer):
        for at in range(half):
            counts = []
            for c in range(chunks):
                reach = 2 if c < DIRECT[layer] else 1
                count = half
                for before, after in ((at, half - 1 - at), (half - 1 - at, at)):
                    count += min(reach, after) + (max(before - reach + 1, 0) if after else 0)
                counts.append(count)
            pl.when(z == at)(functools.partial(x_sent, layer, counts))

    def w_part(layer, device, which):
        size = depth // 2
        return w[layer].at[pl.ds(pl.multiple_of(device * depth + which * size, size), size)]

    def w_send(layer, ref, sem, target):
        remote(ref, ref, ws_sem.at[layer], wr_sem.at[layer, sem], (target, tp)).start()

    def w_start(layer, parts=(0, 1, 2, 3)):
        if not square:
            if 0 in parts:
                for target in sp_peers:
                    w_send(layer, w[layer].at[mine], 2, target)
            return
        plan = ((0, 0, near_x), (1, 1, near_y), (1, 2, near_x), (0, 2, near_y))
        for part in parts:
            which, sem, target = plan[part]
            w_send(layer, w_part(layer, sp, which), sem, target)

    def w_relay(layer, along=(0, 1)):
        if not square:
            return
        for which in along:
            source, target = ((near_x, near_y), (near_y, near_x))[which]
            ref = w_part(layer, source, which)
            sem = wr_sem.at[layer, which]
            remote(ref, ref, ws_sem.at[layer], sem, (source, tp)).wait_recv()
            w_send(layer, ref, 2, target)

    def w_all(layer, blocks):
        ref = w[layer].at[pl.ds(0, blocks * depth)]
        return remote(ref, ref, ws_sem.at[layer], wr_sem.at[layer, 2], (sp, partner))

    def halo(layer, way, row):
        buf = kvp[layer]
        target = lax.rem(sp + (1 if way == 0 else n_sp - 1), n_sp)
        at = low + row * GRID_W
        index = row - (rows_dev - HALO) if way == 0 else HALO + row
        return remote(
            buf.at[pl.ds(at, GRID_W)],
            buf.at[pl.ds(at + (tokens if way else -tokens), GRID_W)],
            hs_sem.at[layer, way],
            hr_sem.at[layer, index],
            (target, tp),
        )

    receives = (has_previous, has_next)

    def halo_start(layer, c):
        for way, row in halo_plan(rows_dev, layer)[c]:
            pl.when(receives[1 - way])(halo(layer, way, row).start)

    def halo_wait(layer, way, rows):
        pl.when(receives[way])(lambda: [halo(layer, way, row).wait_recv() for row in rows] and None)

    def halo_sent(layer, way):
        ref = kvp[layer].at[pl.ds(0, (low, below)[way])]
        copy = remote(ref, ref, hs_sem.at[layer, way], hr_sem.at[layer, 0], (sp, partner))
        pl.when(receives[1 - way])(copy.wait_send)

    def norm(layer, c):
        buf = xg[layer]
        for row in orders[layer][c]:
            at = pl.ds(place(layer, row), GRID_W)
            start = flat[layer].index(row) * GRID_W
            to = pl.ds(start, GRID_W)
            total = jnp.zeros((GRID_W, feat), jnp.float32)
            for s in range(n_tp):
                wide = buf[s, at, :].astype(jnp.float32)
                total = total + wide * wide
            mean = jnp.sum(total, axis=-1, keepdims=True) * (1.0 / (n_tp * feat))
            scale = lax.rsqrt(mean + epsilon)
            for s in range(n_tp):
                slot = slot_of(s % 2, s // 2)
                gain = xg_a[slot, 0:GAIN_ROWS, :][layer : layer + 1, :]
                wide = buf[slot, at, :].astype(jnp.float32)
                normed[to, s * feat : (s + 1) * feat] = (
                    wide * scale * gain.astype(jnp.float32)
                ).astype(jnp.bfloat16)

    def project(layer, c):
        chunk = orders[layer][c]
        at = flat[layer].index(chunk[0]) * GRID_W
        made = jnp.dot(
            normed[at : at + len(chunk) * GRID_W, :],
            w[layer][...],
            preferred_element_type=jnp.float32,
        ).astype(jnp.bfloat16)
        for i, row in enumerate(chunk):
            part = made[i * GRID_W : (i + 1) * GRID_W]
            to = row * GRID_W
            kvp[layer][low + to : low + to + GRID_W, :] = part[:, 0 : 2 * feat]
            q_buf[to : to + GRID_W, :] = part[:, 2 * feat : 3 * feat]
        halo_start(layer, c)

    def attend(layer, indices):
        places, scores = [], []
        for index in indices:
            row = sp * rows_dev + index
            first = jnp.minimum(jnp.maximum(row - HALO, 0), total_rows - WIN_R)
            local = first - sp * rows_dev + HALO
            base = first - row + WIN_R - 1
            at = pl.ds(pl.multiple_of(local * GRID_W, GRID_W), WIN_R * GRID_W)
            query = q_buf[index * GRID_W : (index + 1) * GRID_W, :]
            raw = lax.dot_general(
                query,
                kvp[layer][at, 0:feat],
                (((1,), (1,)), ((), ())),
                preferred_element_type=jnp.float32,
            )
            bias = jnp.concatenate([tiles[layer][base + 2 * j] for j in range(WIN_R // 2)], axis=1)
            places.append(at)
            scores.append(raw * factor + bias)
        tops = [jnp.max(score, axis=-1, keepdims=True) for score in scores]
        weights = [jnp.exp(score - top) for score, top in zip(scores, tops)]
        scales = [1.0 / jnp.sum(weight, axis=-1, keepdims=True) for weight in weights]
        outs = [
            jnp.dot(
                (weight * scale).astype(jnp.bfloat16),
                kvp[layer][at, feat : 2 * feat],
                preferred_element_type=jnp.float32,
            )
            for weight, scale, at in zip(weights, scales, places)
        ]
        made = []
        for index, out in zip(indices, outs):
            wide = xg[layer][own, pl.ds(place(layer, index), GRID_W), :].astype(jnp.float32)
            made.append((wide + out).astype(jnp.bfloat16))
        return made

    sync = 1 + has_right.astype(jnp.int32) + has_left.astype(jnp.int32)
    sync += 2 + crossed.astype(jnp.int32) if square else n_sp - 1
    pl.semaphore_wait(barrier, sync)
    loaded(0, xg_a.at[own, pl.ds(GAIN_ROWS, tokens)])
    for c in range(chunks):
        x_start(0, c)
    loaded(1, w_a.at[mine])
    w_start(0)
    loaded(5, tables_buf.at[0])
    loaded(6, tables_buf.at[1])
    build_bias(tables_buf.at[0], rows_buf, tiles_a)
    build_bias(tables_buf.at[1], rows_buf, tiles_b)
    loaded(2, w_b.at[mine])

    last = half - 1

    def lead_end(layer):
        if layer == 0:
            for c in range(chunks):
                x_take(layer, c, 1)
            w_relay(0)
            w_start(1, (0,))

    def end_take(layer, c):
        for k in range(2 - layer, last + 1):
            x_take(layer, c, k)

    def lead_middle(layer):
        for c in range(min(DIRECT[layer], chunks)):
            for k in range(1, last + 1):
                x_take(layer, c, k)
        for k in range(1, last + 1, 2):
            for c in range(DIRECT[layer], chunks):
                for one in range(k, min(k + 2, last + 1)):
                    x_take(layer, c, one)
            if k == 1 and layer == 0:
                w_relay(0)
        if layer == 0:
            w_start(1, (0,))

    for layer in range(2):
        pl.when(is_end)(functools.partial(lead_end, layer))
        if half > 2:
            pl.when(jnp.logical_not(is_end))(functools.partial(lead_middle, layer))
        lag = LAG[layer]
        for c in range(chunks + lag):
            if c < chunks:
                pl.when(is_end)(functools.partial(end_take, layer, c))
            if c < lag:
                continue
            x_finish(layer, c - lag)
            norm(layer, c - lag)
            if c == lag:
                if layer == 0 and square:
                    w_start(1, (1, 3))
                w_all(layer, 2 if square else n_sp - 1).wait_recv()
            project(layer, c - lag)

        finished, sent = set(), 0
        groups = row_groups(rows_dev, layer)
        for step, (waits, rows) in enumerate(groups):
            if layer == 0 and step == min(W_STEP, len(groups) - 1):
                if square:
                    w_start(1, (2,))
                w_relay(1)
            for way in range(2):
                asked = [row for each, row in waits if each == way]
                if asked:
                    halo_wait(layer, way, asked)
            for at in range(0, len(rows), BATCH):
                batch = rows[at : at + BATCH]
                for index, made in zip(batch, attend(layer, batch)):
                    if layer == 1:
                        out_ref[index * GRID_W : (index + 1) * GRID_W, :] = made
                    else:
                        xg_b[own, pl.ds(place(1, index), GRID_W), :] = made
                        finished.add(index)
                while layer == 0 and sent < chunks:
                    if not set(orders[1][sent]) <= finished:
                        break
                    x_start(1, sent)
                    sent += 1

    for layer in range(2):
        for way in range(2):
            halo_sent(layer, way)
        w_all(layer, n_sp - 1).wait_send()
        x_drain(layer)


def body(n_sp, n_tp, stream, gain_a, wq_a, wk_a, wv_a, table_a, gain_b, wq_b, wk_b, wv_b, table_b):
    tokens, feat = stream.shape
    depth = wq_a.shape[0] * n_sp
    rows_dev = tokens // GRID_W
    chunks = len(row_orders(rows_dev)[0])
    bf16 = jnp.bfloat16
    padded = tokens + 2 * HALO * GRID_W
    hbm = pl.BlockSpec(memory_space=pl.ANY)
    vmem = pl.BlockSpec(memory_space=pltpu.VMEM)
    dma = pltpu.SemaphoreType.DMA
    return pl.pallas_call(
        functools.partial(kernel, n_sp, n_tp),
        out_shape=pltpu.VMEM((tokens, feat), bf16),
        in_specs=[hbm] * 11,
        out_specs=vmem,
        scratch_shapes=[
            pltpu.VMEM((n_tp, tokens + GAIN_ROWS, feat), bf16),
            pltpu.VMEM((n_tp, tokens, feat), bf16),
            pltpu.VMEM((depth, 3 * feat), bf16),
            pltpu.VMEM((depth, 3 * feat), bf16),
            pltpu.VMEM((padded, 2 * feat), bf16),
            pltpu.VMEM((padded, 2 * feat), bf16),
            pltpu.VMEM((tokens, feat), bf16),
            pltpu.VMEM((tokens, n_tp * feat), bf16),
            pltpu.VMEM((2, 1, feat), bf16),
            pltpu.VMEM((2, 2 * WIN_R - 1, 1, 2 * WIN_C - 1), jnp.float32),
            pltpu.VMEM((2 * WIN_R, 2 * GRID_W), jnp.float32),
            pltpu.VMEM((2 * WIN_R - 2, GRID_W, 2 * GRID_W), jnp.float32),
            pltpu.VMEM((2 * WIN_R - 2, GRID_W, 2 * GRID_W), jnp.float32),
            dma((7,)),
            dma((2,)),
            dma((2, chunks, n_tp // 2 - 1)),
            dma((2, chunks)),
            dma((2,)),
            dma((2, 3)),
            dma((2, 2)),
            dma((2, 2 * HALO)),
        ],
        compiler_params=pltpu.CompilerParams(collective_id=0, has_side_effects=True),
    )(
        stream,
        gain_a.reshape(1, feat),
        gain_b.reshape(1, feat),
        wq_a,
        wk_a,
        wv_a,
        wq_b,
        wk_b,
        wv_b,
        jnp.transpose(table_a, (1, 0, 2)),
        jnp.transpose(table_b, (1, 0, 2)),
    )


def solution(mesh):
    placed = (
        P("sp", "tp"),
        P("tp"),
        P("sp", "tp"),
        P("sp", "tp"),
        P("sp", "tp"),
        P("tp", None, None),
        P("tp"),
        P("sp", "tp"),
        P("sp", "tp"),
        P("sp", "tp"),
        P("tp", None, None),
    )
    return jax.shard_map(
        functools.partial(body, mesh.shape["sp"], mesh.shape["tp"]),
        mesh=mesh,
        in_specs=placed,
        out_specs=P("sp", "tp"),
        check_vma=False,
    )
```

```python
import functools

import jax
import jax.numpy as jnp
from jax import lax
from jax.experimental import pallas as pl
from jax.experimental.pallas import tpu as pltpu
from jax.sharding import PartitionSpec as P

GRID_W = 64
WIN_R = 8
WIN_C = 16
HALO = 4
GAIN_ROWS = 16
LAG = (2, 1)
EAGER = (1, 0)
DIRECT = (1, 4)
ENDS = (1, 1)
DEFER = ((0, 0, 0, 0), (1, 2, 3, 0))
BATCH = 5
W_STEP = 2
W_EARLY = 0
SWAP = (False, True)
PACE = (1, 2, 3)
epsilon = 1e-06
MESH = pl.DeviceIdType.MESH


def build_bias(table_ref, rows_ref, tiles_ref):
    rows_ref[...] = jnp.zeros_like(rows_ref)
    rows_ref[0 : 2 * WIN_R - 1, 0 : 2 * WIN_C - 1] = table_ref[:, 0, :]
    shape = (GRID_W, 2 * GRID_W)
    column = lax.broadcasted_iota(jnp.int32, shape, 0)
    key_column = lax.broadcasted_iota(jnp.int32, shape, 1)
    key_column = jnp.where(key_column >= GRID_W, key_column - GRID_W, key_column)
    start = jnp.clip(column - WIN_C // 2, 0, GRID_W - WIN_C)
    inside = (key_column >= start) & (key_column < start + WIN_C)
    for o in range(2 * WIN_R - 2):
        pair = rows_ref[o : o + 1, :] + pltpu.roll(rows_ref[o + 1 : o + 2, :], GRID_W, 1)
        tile = pltpu.roll(
            jnp.broadcast_to(pair, shape), 2 * GRID_W - (WIN_C - 1), 1, stride=1, stride_axis=0
        )
        tiles_ref[o] = jnp.where(inside, tile, -1e30)


def row_orders(rows_dev):
    if rows_dev < WIN_R:
        each = [[r] for r in range(rows_dev)]
        return (each, each)
    edge, last = rows_dev - HALO, rows_dev - 1
    inner = list(range(HALO - 1, edge))
    first = [[0, last], [1, last - 1], [2, last - 2], inner + [edge]]
    second = [inner + [edge, edge + 1], [2, last - 1], [1, last], [0]]
    return (first, second)


def halo_plan(rows_dev, layer):
    below = HALO - 1 if rows_dev >= WIN_R else HALO
    edge, plan = rows_dev - HALO, []
    for chunk in row_orders(rows_dev)[layer]:
        up = [(1, row) for row in chunk if row < below]
        plan.append(up + [(0, row) for row in chunk if row >= edge])
    if rows_dev < WIN_R:
        return plan
    late = DEFER[layer]
    held = []
    for c, sends in enumerate(plan):
        ups = [send for send in sends if send[0] == 1]
        downs = held + [send for send in sends if send[0] == 0]
        held = downs[max(len(downs) - late[c], 0) :]
        plan[c] = ups + downs[: max(len(downs) - late[c], 0)]
    return plan


def row_groups(rows_dev, layer):
    every = list(range(rows_dev))
    below = HALO - 1 if rows_dev >= WIN_R else HALO
    edge, last = rows_dev - HALO, rows_dev - 1
    up = [(1, r) for r in range(below)]
    down = [(0, r) for r in range(edge, rows_dev)]
    if rows_dev < WIN_R:
        return [(up + down, every)]
    if layer == 0:
        return [
            ([(1, 0), (0, last)], every[3 : edge + 2]),
            ([(1, 1), (0, last - 1)], [2, last - 1]),
            ([(1, 2), (0, last - 2)], [1, last]),
            ([(0, edge)], [0]),
        ]
    return [([], [edge]), (up, every[edge + 1 :]), (down, every[:edge])]


def kernel(
    n_sp,
    n_tp,
    x_ref,
    gain_a,
    gain_b,
    wq_a,
    wk_a,
    wv_a,
    wq_b,
    wk_b,
    wv_b,
    table_a,
    table_b,
    out_ref,
    xg_a,
    xg_b,
    w_a,
    w_b,
    kvp_a,
    kvp_b,
    q_buf,
    normed,
    gains_buf,
    tables_buf,
    rows_buf,
    tiles_a,
    tiles_b,
    load_sem,
    send_sem,
    xr_sem,
    xp_sem,
    wr_sem,
    hr_sem,
):
    sp = lax.axis_index("sp")
    tp = lax.axis_index("tp")
    tokens, feat = x_ref.shape
    depth = wq_a.shape[0]
    rows_dev = tokens // GRID_W
    total_rows = rows_dev * n_sp
    half = n_tp // 2
    core = lax.rem(tp, 2)
    z = tp // 2
    partner = tp + 1 - 2 * core
    low = HALO * GRID_W
    below_rows = HALO - 1 if rows_dev >= WIN_R else HALO
    below = below_rows * GRID_W
    factor = feat ** (-0.5)
    orders = row_orders(rows_dev)
    counts = [len(order) for order in orders]

    xg = (xg_a, xg_b)
    w = (w_a, w_b)
    kvp = (kvp_a, kvp_b)
    tiles = (tiles_a, tiles_b)

    square = n_sp == 4
    near_x = sp + 1 - 2 * lax.rem(sp, 2)
    near_y = lax.rem(sp + 2, n_sp)
    sp_peers = [lax.rem(sp + k, n_sp) for k in range(1, n_sp)]
    has_next = sp < n_sp - 1
    has_previous = sp > 0
    has_right = z < half - 1
    has_left = z > 0
    is_end = jnp.logical_not(has_left & has_right)
    crossed = (sp == 1) | (sp == 2)

    barrier = pltpu.get_barrier_semaphore()

    def greet(s, t):
        pl.semaphore_signal(barrier, inc=1, device_id=(s, t), device_id_type=MESH)

    pl.when(has_right)(lambda: greet(sp, tp + 2))
    pl.when(has_left)(lambda: greet(sp, tp - 2))
    if DIRECT[0] and half > 2:
        pl.when(z == half - 3)(lambda: greet(sp, tp + 4))
        if ENDS[0] == 1:
            pl.when(z == 2)(lambda: greet(sp, tp - 4))
    for s in (near_x, near_y) if square else sp_peers:
        greet(s, tp)
    if square:
        pl.when(crossed)(lambda: greet(3 - sp, tp))
    greet(sp, partner)

    def slot_of(c, j):
        return c * half + j

    own = slot_of(core, z)

    def w_rows(device):
        return pl.ds(pl.multiple_of(device * depth, depth), depth)

    mine = w_rows(sp)

    flat = [[row for chunk in order for row in chunk] for order in orders]

    def place(layer, row):
        return flat[layer].index(row) * GRID_W + (GAIN_ROWS if layer == 0 else 0)

    def span(layer, c):
        at, size = place(layer, orders[layer][c][0]), len(orders[layer][c]) * GRID_W
        if layer == 0 and c == 0:
            return pl.ds(0, size + GAIN_ROWS)
        return pl.ds(at, size)

    runs = []
    for row in flat[0]:
        if runs and runs[-1][-1] == row - 1:
            runs[-1].append(row)
        else:
            runs.append([row])
    for run in runs:
        pltpu.make_async_copy(
            x_ref.at[pl.ds(run[0] * GRID_W, len(run) * GRID_W)],
            xg_a.at[own, pl.ds(place(0, run[0]), len(run) * GRID_W)],
            load_sem.at[0],
        ).start()
    loads = [
        (1, wk_a, w_a.at[mine, pl.ds(0, feat)]),
        (1, wv_a, w_a.at[mine, pl.ds(feat, feat)]),
        (1, wq_a, w_a.at[mine, pl.ds(2 * feat, feat)]),
        (3, gain_a, gains_buf.at[0]),
        (3, gain_b, gains_buf.at[1]),
        (4, table_a, tables_buf.at[0]),
        (4, table_b, tables_buf.at[1]),
        (2, wk_b, w_b.at[mine, pl.ds(0, feat)]),
        (2, wv_b, w_b.at[mine, pl.ds(feat, feat)]),
        (2, wq_b, w_b.at[mine, pl.ds(2 * feat, feat)]),
    ]
    for i, src, dst in loads:
        pltpu.make_async_copy(src, dst, load_sem.at[i]).start()

    def loaded(i, ref):
        pltpu.make_async_copy(ref, ref, load_sem.at[i]).wait()

    loaded(3, gains_buf)
    spare = jnp.zeros((GAIN_ROWS - 2, feat), jnp.float32)
    both = [gains_buf[0].astype(jnp.float32), gains_buf[1].astype(jnp.float32), spare]
    xg_a[own, 0:GAIN_ROWS, :] = jnp.concatenate(both, axis=0).astype(jnp.bfloat16)

    def remote(src, dst, send, recv, device):
        return pltpu.make_async_remote_copy(
            src_ref=src,
            dst_ref=dst,
            send_sem=send,
            recv_sem=recv,
            device_id=device,
            device_id_type=MESH,
        )

    def x_copy(layer, c, j, target):
        ref = xg[layer].at[slot_of(core, j), span(layer, c)]
        index = lax.rem(j - target + half, half) - 1
        device = (sp, 2 * target + core)
        return remote(ref, ref, send_sem, xr_sem.at[layer, c, index], device)

    def x_pass(layer, c, j):
        ref = xg[layer].at[slot_of(core, j), span(layer, c)]
        return remote(ref, ref, send_sem, xp_sem.at[layer, c], (sp, partner))

    def reaches(layer, c, j):
        senders = (True, (j == 0) | (j == half - 1), j == half - 1)[ENDS[layer]]
        return (c < DIRECT[layer]) & senders

    def x_start(layer, c):
        for far in (2, 1)[c >= DIRECT[layer] :]:
            allowed = reaches(layer, c, z) if far == 2 else True
            pl.when((z + far < half) & allowed)(
                lambda far=far: x_copy(layer, c, z, z + far).start()
            )
            pl.when((z - far >= 0) & allowed)(
                lambda far=far: x_copy(layer, c, z, z - far).start()
            )
        x_pass(layer, c, z).start()

    both_sides = jnp.minimum(z, half - 1 - z)
    far = jnp.where(2 * z < half, 1, -1)

    def source(k):
        paired = k <= 2 * both_sides
        away = jnp.where(paired, (k + 1) // 2, k - both_sides)
        side = far if k % 2 else jnp.where(paired, -far, far)
        return z + away * side, side, away

    sources = [source(k) for k in range(1, half)]

    def x_take(layer, c, k):
        j, side, away = sources[k - 1]
        index = lax.rem(j - z + half, half) - 1
        ref = xg[layer].at[slot_of(core, j), span(layer, c)]
        remote(ref, ref, send_sem, xr_sem.at[layer, c, index], (sp, partner)).wait_recv()
        onward = jnp.where(side > 0, has_left, has_right)
        if c < DIRECT[layer]:
            onward &= (away >= 2) | jnp.logical_not(reaches(layer, c, j))
        pl.when(onward)(lambda: x_copy(layer, c, j, z - side).start())
        x_pass(layer, c, j).start()

    def x_finish(layer, c):
        ref = xg[layer].at[pl.ds((1 - core) * half, half), span(layer, c)]
        remote(ref, ref, send_sem, xp_sem.at[layer, c], (sp, partner)).wait_recv()

    def x_sent(layer, totals):
        for c, count in enumerate(totals):
            for part in [n_tp] * (count // n_tp) + [count % n_tp] * (count % n_tp > 0):
                ref = xg[layer].at[pl.ds(0, part), span(layer, c)]
                sems = send_sem, xp_sem.at[layer, 0]
                remote(ref, ref, *sems, (sp, partner)).wait_send()

    def x_drain(layer):
        for at in range(half):
            totals = []
            for c in range(counts[layer]):
                count = half
                for j in range(half):
                    direct = bool(reaches(layer, c, j))
                    for way in (-1, 1):
                        if not 0 <= at + way < half or (at - j) * way < 0:
                            continue
                        count += not (direct and abs(at - j) == 1)
                        count += direct and j == at and 0 <= at + 2 * way < half
                totals.append(count)
            pl.when(z == at)(functools.partial(x_sent, layer, totals))

    def w_part(layer, device, which):
        size = depth // 2
        return w[layer].at[pl.ds(pl.multiple_of(device * depth + which * size, size), size)]

    def w_send(layer, ref, sem, target):
        remote(ref, ref, send_sem, wr_sem.at[layer, sem], (target, tp)).start()

    def w_start(layer, parts=(0, 1, 2, 3)):
        if not square:
            if 0 in parts:
                for target in sp_peers:
                    w_send(layer, w[layer].at[mine], 2, target)
            return
        plan = ((0, 0, near_x), (1, 1, near_y), (1, 2, near_x), (0, 2, near_y))
        for part in parts:
            which, sem, target = plan[part]
            w_send(layer, w_part(layer, sp, which), sem, target)

    def w_relay(layer, along=(0, 1)):
        if not square:
            return
        for which in along:
            source, target = ((near_x, near_y), (near_y, near_x))[which]
            ref = w_part(layer, source, which)
            sem = wr_sem.at[layer, which]
            remote(ref, ref, send_sem, sem, (source, tp)).wait_recv()
            w_send(layer, ref, 2, target)

    def w_all(layer, blocks):
        ref = w[layer].at[pl.ds(0, blocks * depth)]
        return remote(ref, ref, send_sem, wr_sem.at[layer, 2], (sp, partner))

    def halo(layer, way, row):
        buf = kvp[layer]
        target = lax.rem(sp + (1 if way == 0 else n_sp - 1), n_sp)
        at = low + row * GRID_W
        index = row - (rows_dev - HALO) if way == 0 else HALO + row
        if layer == 1:
            index = 2 * HALO + way
        return remote(
            buf.at[pl.ds(at, GRID_W)],
            buf.at[pl.ds(at + (tokens if way else -tokens), GRID_W)],
            send_sem,
            hr_sem.at[index],
            (target, tp),
        )

    receives = (has_previous, has_next)

    def halo_start(layer, c):
        for way, row in halo_plan(rows_dev, layer)[c]:
            pl.when(receives[1 - way])(halo(layer, way, row).start)

    def halo_wait(layer, way, rows):
        if layer == 0:
            copies = [halo(layer, way, row) for row in rows]
        else:
            at, size = ((0, low), (low + tokens, below))[way]
            ref = kvp[layer].at[pl.ds(at, size)]
            copies = [remote(ref, ref, send_sem, hr_sem.at[2 * HALO + way], (sp, partner))]

        def wait():
            for copy in copies:
                copy.wait_recv()

        pl.when(receives[way])(wait)

    def halo_sent(layer, way):
        ref = kvp[layer].at[pl.ds(0, (low, below)[way])]
        copy = remote(ref, ref, send_sem, hr_sem.at[0], (sp, partner))
        pl.when(receives[1 - way])(copy.wait_send)

    def norm(layer, c):
        buf = xg[layer]
        for row in orders[layer][c]:
            at = pl.ds(place(layer, row), GRID_W)
            start = flat[layer].index(row) * GRID_W
            to = pl.ds(start, GRID_W)
            total = jnp.zeros((GRID_W, feat), jnp.float32)
            for s in range(n_tp):
                wide = buf[s, at, :].astype(jnp.float32)
                total = total + wide * wide
            mean = jnp.sum(total, axis=-1, keepdims=True) * (1.0 / (n_tp * feat))
            scale = lax.rsqrt(mean + epsilon)
            for s in range(n_tp):
                slot = slot_of(s % 2, s // 2)
                gain = xg_a[slot, 0:GAIN_ROWS, :][layer : layer + 1, :]
                wide = buf[slot, at, :].astype(jnp.float32)
                normed[to, s * feat : (s + 1) * feat] = (
                    wide * scale * gain.astype(jnp.float32)
                ).astype(jnp.bfloat16)

    def project(layer, c):
        chunk = orders[layer][c]
        at = flat[layer].index(chunk[0]) * GRID_W
        made = jnp.dot(
            normed[at : at + len(chunk) * GRID_W, :],
            w[layer][...],
            preferred_element_type=jnp.float32,
        ).astype(jnp.bfloat16)
        for i, row in enumerate(chunk):
            part = made[i * GRID_W : (i + 1) * GRID_W]
            to = row * GRID_W
            kvp[layer][low + to : low + to + GRID_W, :] = part[:, 0 : 2 * feat]
            q_buf[to : to + GRID_W, :] = part[:, 2 * feat : 3 * feat]
        halo_start(layer, c)

    def attend(layer, indices):
        places, scores = [], []
        for index in indices:
            row = sp * rows_dev + index
            first = jnp.minimum(jnp.maximum(row - HALO, 0), total_rows - WIN_R)
            local = first - sp * rows_dev + HALO
            base = first - row + WIN_R - 1
            at = pl.ds(pl.multiple_of(local * GRID_W, GRID_W), WIN_R * GRID_W)
            query = q_buf[index * GRID_W : (index + 1) * GRID_W, :]
            raw = lax.dot_general(
                query,
                kvp[layer][at, 0:feat],
                (((1,), (1,)), ((), ())),
                preferred_element_type=jnp.float32,
            )
            bias = jnp.concatenate([tiles[layer][base + 2 * j] for j in range(WIN_R // 2)], axis=1)
            places.append(at)
            scores.append(raw * factor + bias)
        tops = [jnp.max(score, axis=-1, keepdims=True) for score in scores]
        weights = [jnp.exp(score - top) for score, top in zip(scores, tops)]
        scales = [1.0 / jnp.sum(weight, axis=-1, keepdims=True) for weight in weights]
        outs = [
            jnp.dot(
                (weight * scale).astype(jnp.bfloat16),
                kvp[layer][at, feat : 2 * feat],
                preferred_element_type=jnp.float32,
            )
            for weight, scale, at in zip(weights, scales, places)
        ]
        made = []
        for index, out in zip(indices, outs):
            wide = xg[layer][own, pl.ds(place(layer, index), GRID_W), :].astype(jnp.float32)
            made.append((wide + out).astype(jnp.bfloat16))
        return made

    sync = 1 + has_right.astype(jnp.int32) + has_left.astype(jnp.int32)
    sync += 2 + crossed.astype(jnp.int32) if square else n_sp - 1
    if DIRECT[0] and half > 2:
        sync += (z == half - 1).astype(jnp.int32)
        if ENDS[0] == 1:
            sync += (z == 0).astype(jnp.int32)
    pl.semaphore_wait(barrier, sync)
    loaded(0, xg_a.at[own, pl.ds(GAIN_ROWS, tokens)])
    x_start(0, 0)
    spread = [min(at, counts[0]) for at in PACE]
    for c in range(spread[0], spread[1]):
        x_start(0, c)
    loaded(1, w_a.at[mine])
    w_start(0)
    loaded(4, tables_buf)
    build_bias(tables_buf.at[0], rows_buf, tiles_a)
    for c in range(spread[1], spread[2]):
        x_start(0, c)
    build_bias(tables_buf.at[1], rows_buf, tiles_b)
    for c in range(spread[2], counts[0]):
        x_start(0, c)
    loaded(2, w_b.at[mine])

    last = half - 1

    def lead_end(layer):
        if layer == 0:
            for c in range(counts[0]):
                x_take(layer, c, 1)
            w_relay(0)
            w_start(1, (0,))

    def end_take(layer, c):
        for k in range(2 - layer, last + 1):
            x_take(layer, c, k)

    def lead_middle(layer):
        straight = min(DIRECT[layer], counts[layer])
        late = [2] if SWAP[layer] and last == 3 else []
        for c in range(straight):
            for k in range(1, last + 1):
                if k not in late:
                    x_take(layer, c, k)
        for k in range(1, last + 1, 2):
            for c in range(straight, counts[layer]):
                for one in range(k, min(k + 2, last + 1)):
                    x_take(layer, c, one)
            if k == 1 and layer == 0:
                w_relay(0)
        for c in range(straight):
            for k in late:
                x_take(layer, c, k)
        if layer == 0 and W_EARLY == 0:
            w_start(1, (0,))

    def handle(layer, rows):
        for at in range(0, len(rows), BATCH):
            batch = rows[at : at + BATCH]
            for index, made in zip(batch, attend(layer, batch)):
                if layer == 1:
                    out_ref[index * GRID_W : (index + 1) * GRID_W, :] = made
                else:
                    xg_b[own, pl.ds(place(1, index), GRID_W), :] = made

    for layer in range(2):
        pl.when(is_end)(functools.partial(lead_end, layer))
        if half > 2:
            pl.when(jnp.logical_not(is_end))(functools.partial(lead_middle, layer))
        lag, chunks = LAG[layer], counts[layer]
        steps, made = [], 0
        for c in range(chunks):
            steps.append((True, c))
            while made <= (c if made < EAGER[layer] else c - lag):
                steps.append((False, made))
                made += 1
        steps += [(False, c) for c in range(made, chunks)]
        for taking, c in steps:
            if taking:
                pl.when(is_end)(functools.partial(end_take, layer, c))
                continue
            x_finish(layer, c)
            norm(layer, c)
            if c == 0:
                if layer == 0 and square:
                    w_start(1, (1, 3))
                w_all(layer, 2 if square else n_sp - 1).wait_recv()
            project(layer, c)

        finished, sent = set(), 0
        groups = row_groups(rows_dev, layer)
        for step, (waits, rows) in enumerate(groups):
            if layer == 0 and step == W_EARLY - 1 and half > 2:
                pl.when(jnp.logical_not(is_end))(functools.partial(w_start, 1, (0,)))
            if layer == 0 and step == min(W_STEP, len(groups) - 1):
                if square:
                    w_start(1, (2,))
                w_relay(1)
            for way in range(2):
                asked = [row for each, row in waits if each == way]
                if asked:
                    halo_wait(layer, way, asked)
            if layer == 0 or rows_dev < WIN_R:
                handle(layer, rows)
            elif step == 0:
                pl.when(has_previous)(functools.partial(handle, layer, rows))
                ahead = groups[2][1] + rows
                pl.when(jnp.logical_not(has_previous))(functools.partial(handle, layer, ahead))
            elif step == 1:
                handle(layer, rows)
            else:
                pl.when(has_previous)(functools.partial(handle, layer, rows))
            finished |= set(rows)
            while layer == 0 and sent < counts[1]:
                if not set(orders[1][sent]) <= finished:
                    break
                x_start(1, sent)
                sent += 1

    for layer in range(2):
        for way in range(2):
            halo_sent(layer, way)
        w_all(layer, n_sp - 1).wait_send()
        x_drain(layer)


def body(n_sp, n_tp, stream, gain_a, wq_a, wk_a, wv_a, table_a, gain_b, wq_b, wk_b, wv_b, table_b):
    tokens, feat = stream.shape
    depth = wq_a.shape[0] * n_sp
    rows_dev = tokens // GRID_W
    chunks = max(len(order) for order in row_orders(rows_dev))
    bf16 = jnp.bfloat16
    padded = tokens + 2 * HALO * GRID_W
    hbm = pl.BlockSpec(memory_space=pl.ANY)
    vmem = pl.BlockSpec(memory_space=pltpu.VMEM)
    dma = pltpu.SemaphoreType.DMA
    return pl.pallas_call(
        functools.partial(kernel, n_sp, n_tp),
        out_shape=pltpu.VMEM((tokens, feat), bf16),
        in_specs=[hbm] * 11,
        out_specs=vmem,
        scratch_shapes=[
            pltpu.VMEM((n_tp, tokens + GAIN_ROWS, feat), bf16),
            pltpu.VMEM((n_tp, tokens, feat), bf16),
            pltpu.VMEM((depth, 3 * feat), bf16),
            pltpu.VMEM((depth, 3 * feat), bf16),
            pltpu.VMEM((padded, 2 * feat), bf16),
            pltpu.VMEM((padded, 2 * feat), bf16),
            pltpu.VMEM((tokens, feat), bf16),
            pltpu.VMEM((tokens, n_tp * feat), bf16),
            pltpu.VMEM((2, 1, feat), bf16),
            pltpu.VMEM((2, 2 * WIN_R - 1, 1, 2 * WIN_C - 1), jnp.float32),
            pltpu.VMEM((2 * WIN_R, 2 * GRID_W), jnp.float32),
            pltpu.VMEM((2 * WIN_R - 2, GRID_W, 2 * GRID_W), jnp.float32),
            pltpu.VMEM((2 * WIN_R - 2, GRID_W, 2 * GRID_W), jnp.float32),
            dma((5,)),
            dma,
            dma((2, chunks, n_tp // 2 - 1)),
            dma((2, chunks)),
            dma((2, 3)),
            dma((2 * HALO + 2,)),
        ],
        compiler_params=pltpu.CompilerParams(collective_id=0, has_side_effects=True),
    )(
        stream,
        gain_a.reshape(1, feat),
        gain_b.reshape(1, feat),
        wq_a,
        wk_a,
        wv_a,
        wq_b,
        wk_b,
        wv_b,
        jnp.transpose(table_a, (1, 0, 2)),
        jnp.transpose(table_b, (1, 0, 2)),
    )


def solution(mesh):
    placed = (
        P("sp", "tp"),
        P("tp"),
        P("sp", "tp"),
        P("sp", "tp"),
        P("sp", "tp"),
        P("tp", None, None),
        P("tp"),
        P("sp", "tp"),
        P("sp", "tp"),
        P("sp", "tp"),
        P("tp", None, None),
    )
    return jax.shard_map(
        functools.partial(body, mesh.shape["sp"], mesh.shape["tp"]),
        mesh=mesh,
        in_specs=placed,
        out_specs=P("sp", "tp"),
        check_vma=False,
    )
```

```python
import functools

import jax
import jax.numpy as jnp
from jax import lax
from jax.experimental import pallas as pl
from jax.experimental.pallas import tpu as pltpu
from jax.sharding import PartitionSpec as P

GRID_W = 64
WIN_R = 8
WIN_C = 16
HALO = 4
GAIN_ROWS = 16
AHEAD = (((1, 4, 4, 4), (1, 4, 4, 4)), ((1, 2, 3, 4), (3, 4, 4, 4)))
DIRECT = (1, 4)
ENDS = (1, 1)
DEFER = ((0, 0, 0, 0), (1, 2, 3, 0))
BATCH = 5
W_STEP = 2
W_EARLY = 0
SWAP = (False, True)
PACE = (1, 2, 3)
epsilon = 1e-06
LOG2E = 1.4426950408889634
MESH = pl.DeviceIdType.MESH


def build_bias(table_ref, rows_ref, tiles_ref):
    rows_ref[...] = jnp.zeros_like(rows_ref)
    rows_ref[0 : 2 * WIN_R - 1, 0 : 2 * WIN_C - 1] = table_ref[:, 0, :]
    shape = (GRID_W, 2 * GRID_W)
    column = lax.broadcasted_iota(jnp.int32, shape, 0)
    key_column = lax.broadcasted_iota(jnp.int32, shape, 1)
    key_column = jnp.where(key_column >= GRID_W, key_column - GRID_W, key_column)
    start = jnp.clip(column - WIN_C // 2, 0, GRID_W - WIN_C)
    inside = (key_column >= start) & (key_column < start + WIN_C)
    for o in range(2 * WIN_R - 2):
        pair = rows_ref[o : o + 1, :] + pltpu.roll(rows_ref[o + 1 : o + 2, :], GRID_W, 1)
        tile = pltpu.roll(
            jnp.broadcast_to(pair, shape), 2 * GRID_W - (WIN_C - 1), 1, stride=1, stride_axis=0
        )
        tiles_ref[o] = jnp.where(inside, tile * LOG2E, -1e30)


def row_orders(rows_dev):
    if rows_dev < WIN_R:
        each = [[r] for r in range(rows_dev)]
        return (each, each)
    edge, last = rows_dev - HALO, rows_dev - 1
    inner = list(range(HALO - 1, edge))
    first = [[0, last], [1, last - 1], [2, last - 2], inner + [edge]]
    second = [inner + [edge, edge + 1], [2, last - 1], [1, last], [0]]
    return (first, second)


def halo_plan(rows_dev, layer):
    below = HALO - 1 if rows_dev >= WIN_R else HALO
    edge, plan = rows_dev - HALO, []
    for chunk in row_orders(rows_dev)[layer]:
        up = [(1, row) for row in chunk if row < below]
        plan.append(up + [(0, row) for row in chunk if row >= edge])
    if rows_dev < WIN_R:
        return plan
    late = DEFER[layer]
    held = []
    for c, sends in enumerate(plan):
        ups = [send for send in sends if send[0] == 1]
        downs = held + [send for send in sends if send[0] == 0]
        held = downs[max(len(downs) - late[c], 0) :]
        plan[c] = ups + downs[: max(len(downs) - late[c], 0)]
    return plan


def row_groups(rows_dev, layer):
    every = list(range(rows_dev))
    below = HALO - 1 if rows_dev >= WIN_R else HALO
    edge, last = rows_dev - HALO, rows_dev - 1
    up = [(1, r) for r in range(below)]
    down = [(0, r) for r in range(edge, rows_dev)]
    if rows_dev < WIN_R:
        return [(up + down, every)]
    if layer == 0:
        return [
            ([(1, 0), (0, last)], every[3 : edge + 2]),
            ([(1, 1), (0, last - 1)], [2, last - 1]),
            ([(1, 2), (0, last - 2)], [1, last]),
            ([(0, edge)], [0]),
        ]
    return [([], [edge]), (up, every[edge + 1 :]), (down, every[:edge])]


def kernel(
    n_sp,
    n_tp,
    x_ref,
    gain_a,
    gain_b,
    wq_a,
    wk_a,
    wv_a,
    wq_b,
    wk_b,
    wv_b,
    table_a,
    table_b,
    out_ref,
    xg_a,
    xg_b,
    w_a,
    w_b,
    kvp_a,
    kvp_b,
    q_buf,
    normed,
    gains_buf,
    tables_buf,
    rows_buf,
    tiles_a,
    tiles_b,
    load_sem,
    send_sem,
    xr_sem,
    xp_sem,
    wr_sem,
    hr_sem,
):
    sp = lax.axis_index("sp")
    tp = lax.axis_index("tp")
    tokens, feat = x_ref.shape
    depth = wq_a.shape[0]
    rows_dev = tokens // GRID_W
    total_rows = rows_dev * n_sp
    half = n_tp // 2
    core = lax.rem(tp, 2)
    z = tp // 2
    partner = tp + 1 - 2 * core
    low = HALO * GRID_W
    below_rows = HALO - 1 if rows_dev >= WIN_R else HALO
    below = below_rows * GRID_W
    factor = feat ** (-0.5) * LOG2E
    orders = row_orders(rows_dev)
    counts = [len(order) for order in orders]

    xg = (xg_a, xg_b)
    w = (w_a, w_b)
    kvp = (kvp_a, kvp_b)
    tiles = (tiles_a, tiles_b)

    square = n_sp == 4
    near_x = sp + 1 - 2 * lax.rem(sp, 2)
    near_y = lax.rem(sp + 2, n_sp)
    sp_peers = [lax.rem(sp + k, n_sp) for k in range(1, n_sp)]
    has_next = sp < n_sp - 1
    has_previous = sp > 0
    has_right = z < half - 1
    has_left = z > 0
    is_end = jnp.logical_not(has_left & has_right)
    crossed = (sp == 1) | (sp == 2)

    barrier = pltpu.get_barrier_semaphore()

    def greet(s, t):
        pl.semaphore_signal(barrier, inc=1, device_id=(s, t), device_id_type=MESH)

    pl.when(has_right)(lambda: greet(sp, tp + 2))
    pl.when(has_left)(lambda: greet(sp, tp - 2))
    if DIRECT[0] and half > 2:
        pl.when(z == half - 3)(lambda: greet(sp, tp + 4))
        if ENDS[0] == 1:
            pl.when(z == 2)(lambda: greet(sp, tp - 4))
    for s in (near_x, near_y) if square else sp_peers:
        greet(s, tp)
    if square:
        pl.when(crossed)(lambda: greet(3 - sp, tp))
    greet(sp, partner)

    def slot_of(c, j):
        return c * half + j

    own = slot_of(core, z)

    def w_rows(device):
        return pl.ds(pl.multiple_of(device * depth, depth), depth)

    mine = w_rows(sp)

    flat = [[row for chunk in order for row in chunk] for order in orders]

    def place(layer, row):
        return flat[layer].index(row) * GRID_W + (GAIN_ROWS if layer == 0 else 0)

    def span(layer, c):
        at, size = place(layer, orders[layer][c][0]), len(orders[layer][c]) * GRID_W
        if layer == 0 and c == 0:
            return pl.ds(0, size + GAIN_ROWS)
        return pl.ds(at, size)

    runs = []
    for row in flat[0]:
        if runs and runs[-1][-1] == row - 1:
            runs[-1].append(row)
        else:
            runs.append([row])
    for run in runs:
        pltpu.make_async_copy(
            x_ref.at[pl.ds(run[0] * GRID_W, len(run) * GRID_W)],
            xg_a.at[own, pl.ds(place(0, run[0]), len(run) * GRID_W)],
            load_sem.at[0],
        ).start()
    loads = [
        (1, wk_a, w_a.at[mine, pl.ds(0, feat)]),
        (1, wv_a, w_a.at[mine, pl.ds(feat, feat)]),
        (1, wq_a, w_a.at[mine, pl.ds(2 * feat, feat)]),
        (3, gain_a, gains_buf.at[0]),
        (3, gain_b, gains_buf.at[1]),
        (4, table_a, tables_buf.at[0]),
        (4, table_b, tables_buf.at[1]),
        (2, wk_b, w_b.at[mine, pl.ds(0, feat)]),
        (2, wv_b, w_b.at[mine, pl.ds(feat, feat)]),
        (2, wq_b, w_b.at[mine, pl.ds(2 * feat, feat)]),
    ]
    for i, src, dst in loads:
        pltpu.make_async_copy(src, dst, load_sem.at[i]).start()

    def loaded(i, ref):
        pltpu.make_async_copy(ref, ref, load_sem.at[i]).wait()

    loaded(3, gains_buf)
    spare = jnp.zeros((GAIN_ROWS - 2, feat), jnp.float32)
    both = [gains_buf[0].astype(jnp.float32), gains_buf[1].astype(jnp.float32), spare]
    xg_a[own, 0:GAIN_ROWS, :] = jnp.concatenate(both, axis=0).astype(jnp.bfloat16)

    def remote(src, dst, send, recv, device):
        return pltpu.make_async_remote_copy(
            src_ref=src,
            dst_ref=dst,
            send_sem=send,
            recv_sem=recv,
            device_id=device,
            device_id_type=MESH,
        )

    def x_copy(layer, c, j, target):
        ref = xg[layer].at[slot_of(core, j), span(layer, c)]
        index = lax.rem(j - target + half, half) - 1
        device = (sp, 2 * target + core)
        return remote(ref, ref, send_sem, xr_sem.at[layer, c, index], device)

    def x_pass(layer, c, j):
        ref = xg[layer].at[slot_of(core, j), span(layer, c)]
        return remote(ref, ref, send_sem, xp_sem.at[layer, c], (sp, partner))

    def reaches(layer, c, j):
        senders = (True, (j == 0) | (j == half - 1), j == half - 1)[ENDS[layer]]
        return (c < DIRECT[layer]) & senders

    def x_start(layer, c):
        for far in (2, 1)[c >= DIRECT[layer] :]:
            allowed = reaches(layer, c, z) if far == 2 else True
            pl.when((z + far < half) & allowed)(
                lambda far=far: x_copy(layer, c, z, z + far).start()
            )
            pl.when((z - far >= 0) & allowed)(
                lambda far=far: x_copy(layer, c, z, z - far).start()
            )
        x_pass(layer, c, z).start()

    both_sides = jnp.minimum(z, half - 1 - z)
    far = jnp.where(2 * z < half, 1, -1)

    def source(k):
        paired = k <= 2 * both_sides
        away = jnp.where(paired, (k + 1) // 2, k - both_sides)
        side = far if k % 2 else jnp.where(paired, -far, far)
        return z + away * side, side, away

    sources = [source(k) for k in range(1, half)]

    def x_take(layer, c, k):
        j, side, away = sources[k - 1]
        index = lax.rem(j - z + half, half) - 1
        ref = xg[layer].at[slot_of(core, j), span(layer, c)]
        remote(ref, ref, send_sem, xr_sem.at[layer, c, index], (sp, partner)).wait_recv()
        onward = jnp.where(side > 0, has_left, has_right)
        if c < DIRECT[layer]:
            onward &= (away >= 2) | jnp.logical_not(reaches(layer, c, j))
        pl.when(onward)(lambda: x_copy(layer, c, j, z - side).start())
        x_pass(layer, c, j).start()

    def x_finish(layer, c):
        ref = xg[layer].at[pl.ds((1 - core) * half, half), span(layer, c)]
        remote(ref, ref, send_sem, xp_sem.at[layer, c], (sp, partner)).wait_recv()

    def x_sent(layer, totals):
        for c, count in enumerate(totals):
            for part in [n_tp] * (count // n_tp) + [count % n_tp] * (count % n_tp > 0):
                ref = xg[layer].at[pl.ds(0, part), span(layer, c)]
                sems = send_sem, xp_sem.at[layer, 0]
                remote(ref, ref, *sems, (sp, partner)).wait_send()

    def x_drain(layer):
        for at in range(half):
            totals = []
            for c in range(counts[layer]):
                count = half
                for j in range(half):
                    direct = bool(reaches(layer, c, j))
                    for way in (-1, 1):
                        if not 0 <= at + way < half or (at - j) * way < 0:
                            continue
                        count += not (direct and abs(at - j) == 1)
                        count += direct and j == at and 0 <= at + 2 * way < half
                totals.append(count)
            pl.when(z == at)(functools.partial(x_sent, layer, totals))

    def w_part(layer, device, which):
        size = depth // 2
        return w[layer].at[pl.ds(pl.multiple_of(device * depth + which * size, size), size)]

    def w_send(layer, ref, sem, target):
        remote(ref, ref, send_sem, wr_sem.at[layer, sem], (target, tp)).start()

    def w_start(layer, parts=(0, 1, 2, 3)):
        if not square:
            if 0 in parts:
                for target in sp_peers:
                    w_send(layer, w[layer].at[mine], 2, target)
            return
        plan = ((0, 0, near_x), (1, 1, near_y), (1, 2, near_x), (0, 2, near_y))
        for part in parts:
            which, sem, target = plan[part]
            w_send(layer, w_part(layer, sp, which), sem, target)

    def w_relay(layer, along=(0, 1)):
        if not square:
            return
        for which in along:
            source, target = ((near_x, near_y), (near_y, near_x))[which]
            ref = w_part(layer, source, which)
            sem = wr_sem.at[layer, which]
            remote(ref, ref, send_sem, sem, (source, tp)).wait_recv()
            w_send(layer, ref, 2, target)

    def w_all(layer, blocks):
        ref = w[layer].at[pl.ds(0, blocks * depth)]
        return remote(ref, ref, send_sem, wr_sem.at[layer, 2], (sp, partner))

    def halo(layer, way, row):
        buf = kvp[layer]
        target = lax.rem(sp + (1 if way == 0 else n_sp - 1), n_sp)
        at = low + row * GRID_W
        index = row - (rows_dev - HALO) if way == 0 else HALO + row
        if layer == 1:
            index = 2 * HALO + way
        return remote(
            buf.at[pl.ds(at, GRID_W)],
            buf.at[pl.ds(at + (tokens if way else -tokens), GRID_W)],
            send_sem,
            hr_sem.at[index],
            (target, tp),
        )

    receives = (has_previous, has_next)

    def halo_start(layer, c):
        for way, row in halo_plan(rows_dev, layer)[c]:
            pl.when(receives[1 - way])(halo(layer, way, row).start)

    def halo_wait(layer, way, rows):
        if layer == 0:
            copies = [halo(layer, way, row) for row in rows]
        else:
            at, size = ((0, low), (low + tokens, below))[way]
            ref = kvp[layer].at[pl.ds(at, size)]
            copies = [remote(ref, ref, send_sem, hr_sem.at[2 * HALO + way], (sp, partner))]

        def wait():
            for copy in copies:
                copy.wait_recv()

        pl.when(receives[way])(wait)

    def halo_sent(layer, way):
        ref = kvp[layer].at[pl.ds(0, (low, below)[way])]
        copy = remote(ref, ref, send_sem, hr_sem.at[0], (sp, partner))
        pl.when(receives[1 - way])(copy.wait_send)

    def norm(layer, c):
        buf = xg[layer]
        for row in orders[layer][c]:
            at = pl.ds(place(layer, row), GRID_W)
            start = flat[layer].index(row) * GRID_W
            to = pl.ds(start, GRID_W)
            total = jnp.zeros((GRID_W, feat), jnp.float32)
            for s in range(n_tp):
                wide = buf[s, at, :].astype(jnp.float32)
                total = total + wide * wide
            mean = jnp.sum(total, axis=-1, keepdims=True) * (1.0 / (n_tp * feat))
            scale = lax.rsqrt(mean + epsilon)
            for s in range(n_tp):
                slot = slot_of(s % 2, s // 2)
                gain = xg_a[slot, 0:GAIN_ROWS, :][layer : layer + 1, :]
                wide = buf[slot, at, :].astype(jnp.float32)
                normed[to, s * feat : (s + 1) * feat] = (
                    wide * scale * gain.astype(jnp.float32)
                ).astype(jnp.bfloat16)

    def project(layer, c):
        chunk = orders[layer][c]
        at = flat[layer].index(chunk[0]) * GRID_W
        made = jnp.dot(
            normed[at : at + len(chunk) * GRID_W, :],
            w[layer][...],
            preferred_element_type=jnp.float32,
        ).astype(jnp.bfloat16)
        for i, row in enumerate(chunk):
            part = made[i * GRID_W : (i + 1) * GRID_W]
            to = row * GRID_W
            kvp[layer][low + to : low + to + GRID_W, :] = part[:, 0 : 2 * feat]
            q_buf[to : to + GRID_W, :] = part[:, 2 * feat : 3 * feat]
        halo_start(layer, c)

    def attend(layer, indices):
        places, scores = [], []
        for index in indices:
            row = sp * rows_dev + index
            first = jnp.minimum(jnp.maximum(row - HALO, 0), total_rows - WIN_R)
            local = first - sp * rows_dev + HALO
            base = first - row + WIN_R - 1
            at = pl.ds(pl.multiple_of(local * GRID_W, GRID_W), WIN_R * GRID_W)
            query = q_buf[index * GRID_W : (index + 1) * GRID_W, :]
            raw = lax.dot_general(
                query,
                kvp[layer][at, 0:feat],
                (((1,), (1,)), ((), ())),
                preferred_element_type=jnp.float32,
            )
            bias = jnp.concatenate([tiles[layer][base + 2 * j] for j in range(WIN_R // 2)], axis=1)
            places.append(at)
            scores.append(raw * factor + bias)
        tops = [jnp.max(score, axis=-1, keepdims=True) for score in scores]
        weights = [jnp.exp2(score - top) for score, top in zip(scores, tops)]
        outs = [
            jnp.dot(
                weight.astype(jnp.bfloat16),
                kvp[layer][at, feat : 2 * feat],
                preferred_element_type=jnp.float32,
            )
            for weight, at in zip(weights, places)
        ]
        scales = [1.0 / jnp.sum(weight, axis=-1, keepdims=True) for weight in weights]
        made = []
        for index, out, scale in zip(indices, outs, scales):
            wide = xg[layer][own, pl.ds(place(layer, index), GRID_W), :].astype(jnp.float32)
            made.append((wide + out * scale).astype(jnp.bfloat16))
        return made

    sync = 1 + has_right.astype(jnp.int32) + has_left.astype(jnp.int32)
    sync += 2 + crossed.astype(jnp.int32) if square else n_sp - 1
    if DIRECT[0] and half > 2:
        sync += (z == half - 1).astype(jnp.int32)
        if ENDS[0] == 1:
            sync += (z == 0).astype(jnp.int32)
    pl.semaphore_wait(barrier, sync)
    loaded(0, xg_a.at[own, pl.ds(GAIN_ROWS, tokens)])
    x_start(0, 0)
    spread = [min(at, counts[0]) for at in PACE]
    for c in range(spread[0], spread[1]):
        x_start(0, c)
    loaded(1, w_a.at[mine])
    w_start(0)
    loaded(4, tables_buf)
    build_bias(tables_buf.at[0], rows_buf, tiles_a)
    for c in range(spread[1], spread[2]):
        x_start(0, c)
    build_bias(tables_buf.at[1], rows_buf, tiles_b)
    for c in range(spread[2], counts[0]):
        x_start(0, c)
    loaded(2, w_b.at[mine])

    last = half - 1

    def lead_end(layer):
        if layer == 0:
            for c in range(counts[0]):
                x_take(layer, c, 1)
            w_relay(0)
            w_start(1, (0,))

    def end_take(layer, c):
        for k in range(2 - layer, last + 1):
            x_take(layer, c, k)

    def lead_middle(layer):
        straight = min(DIRECT[layer], counts[layer])
        late = [2] if SWAP[layer] and last == 3 else []
        for c in range(straight):
            for k in range(1, last + 1):
                if k not in late:
                    x_take(layer, c, k)
        for k in range(1, last + 1, 2):
            for c in range(straight, counts[layer]):
                for one in range(k, min(k + 2, last + 1)):
                    x_take(layer, c, one)
            if k == 1 and layer == 0:
                w_relay(0)
        for c in range(straight):
            for k in late:
                x_take(layer, c, k)
        if layer == 0 and W_EARLY == 0:
            w_start(1, (0,))

    def handle(layer, rows):
        for at in range(0, len(rows), BATCH):
            batch = rows[at : at + BATCH]
            for index, made in zip(batch, attend(layer, batch)):
                if layer == 1:
                    out_ref[index * GRID_W : (index + 1) * GRID_W, :] = made
                else:
                    xg_b[own, pl.ds(place(1, index), GRID_W), :] = made

    for layer in range(2):
        pl.when(is_end)(functools.partial(lead_end, layer))
        if half > 2:
            pl.when(jnp.logical_not(is_end))(functools.partial(lead_middle, layer))
        chunks = counts[layer]
        taken = [0, 0]
        for c in range(chunks):
            for side in range(2):
                stop = min(AHEAD[layer][side][min(c, 3)], chunks) if chunks == 4 else c + 1
                for ask in range(taken[side], stop):
                    mine_now = is_end & (core == side)
                    pl.when(mine_now)(functools.partial(end_take, layer, ask))
                taken[side] = max(taken[side], stop)
            x_finish(layer, c)
            norm(layer, c)
            if c == 0:
                if layer == 0 and square:
                    w_start(1, (1, 3))
                w_all(layer, 2 if square else n_sp - 1).wait_recv()
            project(layer, c)

        if layer == 1 and rows_dev >= WIN_R:
            (_, middle), (up, above), (down, under) = row_groups(rows_dev, layer)
            low_first = sp <= n_sp // 4

            def finish_low():
                handle(layer, under + middle)

            def finish_high():
                handle(layer, middle)

            ask_down = functools.partial(halo_wait, layer, 0, [row for _, row in down])

            def low_side():
                ask_down()
                finish_low()

            def high_side():
                ask_down()
                handle(layer, under)

            pl.when(low_first)(low_side)
            pl.when(jnp.logical_not(low_first))(finish_high)
            halo_wait(layer, 1, [row for _, row in up])
            handle(layer, above)
            pl.when(jnp.logical_not(low_first))(high_side)
            continue

        finished, sent = set(), 0
        groups = row_groups(rows_dev, layer)
        for step, (waits, rows) in enumerate(groups):
            if layer == 0 and step == W_EARLY - 1 and half > 2:
                pl.when(jnp.logical_not(is_end))(functools.partial(w_start, 1, (0,)))
            if layer == 0 and step == min(W_STEP, len(groups) - 1):
                if square:
                    w_start(1, (2,))
                w_relay(1)
            for way in range(2):
                asked = [row for each, row in waits if each == way]
                if asked:
                    halo_wait(layer, way, asked)
            handle(layer, rows)
            finished |= set(rows)
            while layer == 0 and sent < counts[1]:
                if not set(orders[1][sent]) <= finished:
                    break
                x_start(1, sent)
                sent += 1

    for layer in range(2):
        for way in range(2):
            halo_sent(layer, way)
        w_all(layer, n_sp - 1).wait_send()
        x_drain(layer)


def body(n_sp, n_tp, stream, gain_a, wq_a, wk_a, wv_a, table_a, gain_b, wq_b, wk_b, wv_b, table_b):
    tokens, feat = stream.shape
    depth = wq_a.shape[0] * n_sp
    rows_dev = tokens // GRID_W
    chunks = max(len(order) for order in row_orders(rows_dev))
    bf16 = jnp.bfloat16
    padded = tokens + 2 * HALO * GRID_W
    hbm = pl.BlockSpec(memory_space=pl.ANY)
    vmem = pl.BlockSpec(memory_space=pltpu.VMEM)
    dma = pltpu.SemaphoreType.DMA
    return pl.pallas_call(
        functools.partial(kernel, n_sp, n_tp),
        out_shape=pltpu.VMEM((tokens, feat), bf16),
        in_specs=[hbm] * 11,
        out_specs=vmem,
        scratch_shapes=[
            pltpu.VMEM((n_tp, tokens + GAIN_ROWS, feat), bf16),
            pltpu.VMEM((n_tp, tokens, feat), bf16),
            pltpu.VMEM((depth, 3 * feat), bf16),
            pltpu.VMEM((depth, 3 * feat), bf16),
            pltpu.VMEM((padded, 2 * feat), bf16),
            pltpu.VMEM((padded, 2 * feat), bf16),
            pltpu.VMEM((tokens, feat), bf16),
            pltpu.VMEM((tokens, n_tp * feat), bf16),
            pltpu.VMEM((2, 1, feat), bf16),
            pltpu.VMEM((2, 2 * WIN_R - 1, 1, 2 * WIN_C - 1), jnp.float32),
            pltpu.VMEM((2 * WIN_R, 2 * GRID_W), jnp.float32),
            pltpu.VMEM((2 * WIN_R - 2, GRID_W, 2 * GRID_W), jnp.float32),
            pltpu.VMEM((2 * WIN_R - 2, GRID_W, 2 * GRID_W), jnp.float32),
            dma((5,)),
            dma,
            dma((2, chunks, n_tp // 2 - 1)),
            dma((2, chunks)),
            dma((2, 3)),
            dma((2 * HALO + 2,)),
        ],
        compiler_params=pltpu.CompilerParams(collective_id=0, has_side_effects=True),
    )(
        stream,
        gain_a.reshape(1, feat),
        gain_b.reshape(1, feat),
        wq_a,
        wk_a,
        wv_a,
        wq_b,
        wk_b,
        wv_b,
        jnp.transpose(table_a, (1, 0, 2)),
        jnp.transpose(table_b, (1, 0, 2)),
    )


def solution(mesh):
    placed = (
        P("sp", "tp"),
        P("tp"),
        P("sp", "tp"),
        P("sp", "tp"),
        P("sp", "tp"),
        P("tp", None, None),
        P("tp"),
        P("sp", "tp"),
        P("sp", "tp"),
        P("sp", "tp"),
        P("tp", None, None),
    )
    return jax.shard_map(
        functools.partial(body, mesh.shape["sp"], mesh.shape["tp"]),
        mesh=mesh,
        in_specs=placed,
        out_specs=P("sp", "tp"),
        check_vma=False,
    )
```

```python
import functools

import jax
import jax.numpy as jnp
from jax import lax
from jax.experimental import pallas as pl
from jax.experimental.pallas import tpu as pltpu
from jax.sharding import PartitionSpec as P

GRID_W = 64
WIN_R = 8
WIN_C = 16
HALO = 4
GAIN_ROWS = 16
AHEAD = (((1, 4, 4, 4), (1, 4, 4, 4)), ((1, 2, 3, 4), (3, 4, 4, 4)))
DIRECT = (1, 4)
ENDS = (1, 1)
DEFER = ((0, 0, 0, 0), (1, 2, 3, 0))
BATCH = 5
W_STEP = 2
W_EARLY = 0
SWAP = (False, True)
PACE = (1, 2, 3)
epsilon = 1e-06
LOG2E = 1.4426950408889634
MESH = pl.DeviceIdType.MESH


def build_bias(table_ref, rows_ref, tiles_ref):
    rows_ref[...] = jnp.zeros_like(rows_ref)
    rows_ref[0 : 2 * WIN_R - 1, 0 : 2 * WIN_C - 1] = table_ref[:, 0, :]
    shape = (GRID_W, 2 * GRID_W)
    column = lax.broadcasted_iota(jnp.int32, shape, 0)
    key_column = lax.broadcasted_iota(jnp.int32, shape, 1)
    key_column = jnp.where(key_column >= GRID_W, key_column - GRID_W, key_column)
    start = jnp.clip(column - WIN_C // 2, 0, GRID_W - WIN_C)
    inside = (key_column >= start) & (key_column < start + WIN_C)
    for o in range(2 * WIN_R - 2):
        pair = rows_ref[o : o + 1, :] + pltpu.roll(rows_ref[o + 1 : o + 2, :], GRID_W, 1)
        tile = pltpu.roll(
            jnp.broadcast_to(pair, shape), 2 * GRID_W - (WIN_C - 1), 1, stride=1, stride_axis=0
        )
        tiles_ref[o] = jnp.where(inside, tile * LOG2E, -1e30)


def row_orders(rows_dev):
    if rows_dev < WIN_R:
        each = [[r] for r in range(rows_dev)]
        return (each, each)
    edge, last = rows_dev - HALO, rows_dev - 1
    inner = list(range(HALO - 1, edge))
    first = [[0, last], [1, last - 1], [2, last - 2], inner + [edge]]
    second = [inner + [edge, edge + 1], [2, last - 1], [1, last], [0]]
    return (first, second)


def halo_plan(rows_dev, layer):
    below = HALO - 1 if rows_dev >= WIN_R else HALO
    edge, plan = rows_dev - HALO, []
    for chunk in row_orders(rows_dev)[layer]:
        up = [(1, row) for row in chunk if row < below]
        plan.append(up + [(0, row) for row in chunk if row >= edge])
    if rows_dev < WIN_R:
        return plan
    late = DEFER[layer]
    held = []
    for c, sends in enumerate(plan):
        ups = [send for send in sends if send[0] == 1]
        downs = held + [send for send in sends if send[0] == 0]
        held = downs[max(len(downs) - late[c], 0) :]
        plan[c] = ups + downs[: max(len(downs) - late[c], 0)]
    return plan


def row_groups(rows_dev, layer):
    every = list(range(rows_dev))
    below = HALO - 1 if rows_dev >= WIN_R else HALO
    edge, last = rows_dev - HALO, rows_dev - 1
    up = [(1, r) for r in range(below)]
    down = [(0, r) for r in range(edge, rows_dev)]
    if rows_dev < WIN_R:
        return [(up + down, every)]
    if layer == 0:
        return [
            ([(1, 0), (0, last)], every[3 : edge + 2]),
            ([(1, 1), (0, last - 1)], [2, last - 1]),
            ([(1, 2), (0, last - 2)], [1, last]),
            ([(0, edge)], [0]),
        ]
    return [([], [edge]), (up, every[edge + 1 :]), (down, every[:edge])]


def kernel(
    n_sp,
    n_tp,
    x_ref,
    gain_a,
    gain_b,
    wq_a,
    wk_a,
    wv_a,
    wq_b,
    wk_b,
    wv_b,
    table_a,
    table_b,
    out_ref,
    xg_a,
    xg_b,
    w_a,
    w_b,
    kvp_a,
    kvp_b,
    q_buf,
    normed,
    gains_buf,
    tables_buf,
    rows_buf,
    tiles_a,
    tiles_b,
    load_sem,
    send_sem,
    xr_sem,
    xp_sem,
    wr_sem,
    hr_sem,
):
    sp = lax.axis_index("sp")
    tp = lax.axis_index("tp")
    tokens, feat = x_ref.shape
    depth = wq_a.shape[0]
    rows_dev = tokens // GRID_W
    total_rows = rows_dev * n_sp
    half = n_tp // 2
    core = lax.rem(tp, 2)
    z = tp // 2
    partner = tp + 1 - 2 * core
    low = HALO * GRID_W
    below_rows = HALO - 1 if rows_dev >= WIN_R else HALO
    below = below_rows * GRID_W
    factor = feat ** (-0.5) * LOG2E
    orders = row_orders(rows_dev)
    counts = [len(order) for order in orders]

    xg = (xg_a, xg_b)
    w = (w_a, w_b)
    kvp = (kvp_a, kvp_b)
    tiles = (tiles_a, tiles_b)

    square = n_sp == 4
    near_x = sp + 1 - 2 * lax.rem(sp, 2)
    near_y = lax.rem(sp + 2, n_sp)
    sp_peers = [lax.rem(sp + k, n_sp) for k in range(1, n_sp)]
    has_next = sp < n_sp - 1
    has_previous = sp > 0
    has_right = z < half - 1
    has_left = z > 0
    is_end = jnp.logical_not(has_left & has_right)
    crossed = (sp == 1) | (sp == 2)

    barrier = pltpu.get_barrier_semaphore()

    def greet(s, t):
        pl.semaphore_signal(barrier, inc=1, device_id=(s, t), device_id_type=MESH)

    pl.when(has_right)(lambda: greet(sp, tp + 2))
    pl.when(has_left)(lambda: greet(sp, tp - 2))
    if DIRECT[0] and half > 2:
        pl.when(z == half - 3)(lambda: greet(sp, tp + 4))
        if ENDS[0] == 1:
            pl.when(z == 2)(lambda: greet(sp, tp - 4))
    for s in (near_x, near_y) if square else sp_peers:
        greet(s, tp)
    if square:
        pl.when(crossed)(lambda: greet(3 - sp, tp))
    greet(sp, partner)

    def slot_of(c, j):
        return c * half + j

    own = slot_of(core, z)

    def w_rows(device):
        return pl.ds(pl.multiple_of(device * depth, depth), depth)

    mine = w_rows(sp)

    flat = [[row for chunk in order for row in chunk] for order in orders]

    def place(layer, row):
        return flat[layer].index(row) * GRID_W + (GAIN_ROWS if layer == 0 else 0)

    def span(layer, c):
        at, size = place(layer, orders[layer][c][0]), len(orders[layer][c]) * GRID_W
        if layer == 0 and c == 0:
            return pl.ds(0, size + GAIN_ROWS)
        return pl.ds(at, size)

    runs = []
    for row in flat[0]:
        if runs and runs[-1][-1] == row - 1:
            runs[-1].append(row)
        else:
            runs.append([row])
    for run in runs:
        pltpu.make_async_copy(
            x_ref.at[pl.ds(run[0] * GRID_W, len(run) * GRID_W)],
            xg_a.at[own, pl.ds(place(0, run[0]), len(run) * GRID_W)],
            load_sem.at[0],
        ).start()
    loads = [
        (1, wk_a, w_a.at[mine, pl.ds(0, feat)]),
        (1, wv_a, w_a.at[mine, pl.ds(feat, feat)]),
        (1, wq_a, w_a.at[mine, pl.ds(2 * feat, feat)]),
        (3, gain_a, gains_buf.at[0]),
        (3, gain_b, gains_buf.at[1]),
        (4, table_a, tables_buf.at[0]),
        (4, table_b, tables_buf.at[1]),
        (2, wk_b, w_b.at[mine, pl.ds(0, feat)]),
        (2, wv_b, w_b.at[mine, pl.ds(feat, feat)]),
        (2, wq_b, w_b.at[mine, pl.ds(2 * feat, feat)]),
    ]
    for i, src, dst in loads:
        pltpu.make_async_copy(src, dst, load_sem.at[i]).start()

    def loaded(i, ref):
        pltpu.make_async_copy(ref, ref, load_sem.at[i]).wait()

    loaded(3, gains_buf)
    spare = jnp.zeros((GAIN_ROWS - 2, feat), jnp.float32)
    both = [gains_buf[0].astype(jnp.float32), gains_buf[1].astype(jnp.float32), spare]
    xg_a[own, 0:GAIN_ROWS, :] = jnp.concatenate(both, axis=0).astype(jnp.bfloat16)

    def remote(src, dst, send, recv, device):
        return pltpu.make_async_remote_copy(
            src_ref=src,
            dst_ref=dst,
            send_sem=send,
            recv_sem=recv,
            device_id=device,
            device_id_type=MESH,
        )

    def x_copy(layer, c, j, target):
        ref = xg[layer].at[slot_of(core, j), span(layer, c)]
        index = lax.rem(j - target + half, half) - 1
        device = (sp, 2 * target + core)
        return remote(ref, ref, send_sem, xr_sem.at[layer, c, index], device)

    def x_pass(layer, c, j):
        ref = xg[layer].at[slot_of(core, j), span(layer, c)]
        return remote(ref, ref, send_sem, xp_sem.at[layer, c], (sp, partner))

    def reaches(layer, c, j):
        senders = (True, (j == 0) | (j == half - 1), j == half - 1)[ENDS[layer]]
        return (c < DIRECT[layer]) & senders

    def x_start(layer, c):
        for far in (2, 1)[c >= DIRECT[layer] :]:
            allowed = reaches(layer, c, z) if far == 2 else True
            pl.when((z + far < half) & allowed)(
                lambda far=far: x_copy(layer, c, z, z + far).start()
            )
            pl.when((z - far >= 0) & allowed)(
                lambda far=far: x_copy(layer, c, z, z - far).start()
            )
        x_pass(layer, c, z).start()

    both_sides = jnp.minimum(z, half - 1 - z)
    far = jnp.where(2 * z < half, 1, -1)

    def source(k):
        paired = k <= 2 * both_sides
        away = jnp.where(paired, (k + 1) // 2, k - both_sides)
        side = far if k % 2 else jnp.where(paired, -far, far)
        return z + away * side, side, away

    sources = [source(k) for k in range(1, half)]

    def x_take(layer, c, k):
        j, side, away = sources[k - 1]
        index = lax.rem(j - z + half, half) - 1
        ref = xg[layer].at[slot_of(core, j), span(layer, c)]
        remote(ref, ref, send_sem, xr_sem.at[layer, c, index], (sp, partner)).wait_recv()
        onward = jnp.where(side > 0, has_left, has_right)
        if c < DIRECT[layer]:
            onward &= (away >= 2) | jnp.logical_not(reaches(layer, c, j))
        pl.when(onward)(lambda: x_copy(layer, c, j, z - side).start())
        x_pass(layer, c, j).start()

    def x_finish(layer, c):
        ref = xg[layer].at[pl.ds((1 - core) * half, half), span(layer, c)]
        remote(ref, ref, send_sem, xp_sem.at[layer, c], (sp, partner)).wait_recv()

    def x_sent(layer, totals):
        for c, count in enumerate(totals):
            for part in [n_tp] * (count // n_tp) + [count % n_tp] * (count % n_tp > 0):
                ref = xg[layer].at[pl.ds(0, part), span(layer, c)]
                sems = send_sem, xp_sem.at[layer, 0]
                remote(ref, ref, *sems, (sp, partner)).wait_send()

    def x_drain(layer):
        for at in range(half):
            totals = []
            for c in range(counts[layer]):
                count = half
                for j in range(half):
                    direct = bool(reaches(layer, c, j))
                    for way in (-1, 1):
                        if not 0 <= at + way < half or (at - j) * way < 0:
                            continue
                        count += not (direct and abs(at - j) == 1)
                        count += direct and j == at and 0 <= at + 2 * way < half
                totals.append(count)
            pl.when(z == at)(functools.partial(x_sent, layer, totals))

    def w_part(layer, device, which):
        size = depth // 2
        return w[layer].at[pl.ds(pl.multiple_of(device * depth + which * size, size), size)]

    def w_send(layer, ref, sem, target):
        remote(ref, ref, send_sem, wr_sem.at[layer, sem], (target, tp)).start()

    def w_start(layer, parts=(0, 1, 2, 3)):
        if not square:
            if 0 in parts:
                for target in sp_peers:
                    w_send(layer, w[layer].at[mine], 2, target)
            return
        plan = ((0, 0, near_x), (1, 1, near_y), (1, 2, near_x), (0, 2, near_y))
        for part in parts:
            which, sem, target = plan[part]
            w_send(layer, w_part(layer, sp, which), sem, target)

    def w_relay(layer, along=(0, 1)):
        if not square:
            return
        for which in along:
            source, target = ((near_x, near_y), (near_y, near_x))[which]
            ref = w_part(layer, source, which)
            sem = wr_sem.at[layer, which]
            remote(ref, ref, send_sem, sem, (source, tp)).wait_recv()
            w_send(layer, ref, 2, target)

    def w_all(layer, blocks):
        ref = w[layer].at[pl.ds(0, blocks * depth)]
        return remote(ref, ref, send_sem, wr_sem.at[layer, 2], (sp, partner))

    def halo(layer, way, row):
        buf = kvp[layer]
        target = lax.rem(sp + (1 if way == 0 else n_sp - 1), n_sp)
        at = low + row * GRID_W
        index = row - (rows_dev - HALO) if way == 0 else HALO + row
        if layer == 1:
            index = 2 * HALO + way
        return remote(
            buf.at[pl.ds(at, GRID_W)],
            buf.at[pl.ds(at + (tokens if way else -tokens), GRID_W)],
            send_sem,
            hr_sem.at[index],
            (target, tp),
        )

    receives = (has_previous, has_next)

    def halo_start(layer, c):
        for way, row in halo_plan(rows_dev, layer)[c]:
            pl.when(receives[1 - way])(halo(layer, way, row).start)

    def halo_wait(layer, way, rows):
        if layer == 0:
            copies = [halo(layer, way, row) for row in rows]
        else:
            at, size = ((0, low), (low + tokens, below))[way]
            ref = kvp[layer].at[pl.ds(at, size)]
            copies = [remote(ref, ref, send_sem, hr_sem.at[2 * HALO + way], (sp, partner))]

        def wait():
            for copy in copies:
                copy.wait_recv()

        pl.when(receives[way])(wait)

    def halo_sent(layer, way):
        ref = kvp[layer].at[pl.ds(0, (low, below)[way])]
        copy = remote(ref, ref, send_sem, hr_sem.at[0], (sp, partner))
        pl.when(receives[1 - way])(copy.wait_send)

    def norm(layer, c):
        buf = xg[layer]
        for row in orders[layer][c]:
            at = pl.ds(place(layer, row), GRID_W)
            start = flat[layer].index(row) * GRID_W
            to = pl.ds(start, GRID_W)
            total = jnp.zeros((GRID_W, feat), jnp.float32)
            for s in range(n_tp):
                wide = buf[s, at, :].astype(jnp.float32)
                total = total + wide * wide
            mean = jnp.sum(total, axis=-1, keepdims=True) * (1.0 / (n_tp * feat))
            scale = lax.rsqrt(mean + epsilon)
            for s in range(n_tp):
                slot = slot_of(s % 2, s // 2)
                gain = xg_a[slot, 0:GAIN_ROWS, :][layer : layer + 1, :]
                wide = buf[slot, at, :].astype(jnp.float32)
                normed[to, s * feat : (s + 1) * feat] = (
                    wide * scale * gain.astype(jnp.float32)
                ).astype(jnp.bfloat16)

    def project(layer, c):
        chunk = orders[layer][c]
        at = flat[layer].index(chunk[0]) * GRID_W
        made = jnp.dot(
            normed[at : at + len(chunk) * GRID_W, :],
            w[layer][...],
            preferred_element_type=jnp.float32,
        ).astype(jnp.bfloat16)
        for i, row in enumerate(chunk):
            part = made[i * GRID_W : (i + 1) * GRID_W]
            to = row * GRID_W
            kvp[layer][low + to : low + to + GRID_W, :] = part[:, 0 : 2 * feat]
            q_buf[to : to + GRID_W, :] = part[:, 2 * feat : 3 * feat]
        halo_start(layer, c)

    def attend(layer, indices):
        places, scores = [], []
        for index in indices:
            row = sp * rows_dev + index
            first = jnp.minimum(jnp.maximum(row - HALO, 0), total_rows - WIN_R)
            local = first - sp * rows_dev + HALO
            base = first - row + WIN_R - 1
            at = pl.ds(pl.multiple_of(local * GRID_W, GRID_W), WIN_R * GRID_W)
            query = q_buf[index * GRID_W : (index + 1) * GRID_W, :]
            raw = lax.dot_general(
                query,
                kvp[layer][at, 0:feat],
                (((1,), (1,)), ((), ())),
                preferred_element_type=jnp.float32,
            )
            bias = jnp.concatenate([tiles[layer][base + 2 * j] for j in range(WIN_R // 2)], axis=1)
            places.append(at)
            scores.append(raw * factor + bias)
        tops = [jnp.max(score, axis=-1, keepdims=True) for score in scores]
        weights = [jnp.exp2(score - top) for score, top in zip(scores, tops)]
        outs = [
            jnp.dot(
                weight.astype(jnp.bfloat16),
                kvp[layer][at, feat : 2 * feat],
                preferred_element_type=jnp.float32,
            )
            for weight, at in zip(weights, places)
        ]
        scales = [1.0 / jnp.sum(weight, axis=-1, keepdims=True) for weight in weights]
        made = []
        for index, out, scale in zip(indices, outs, scales):
            wide = xg[layer][own, pl.ds(place(layer, index), GRID_W), :].astype(jnp.float32)
            made.append((wide + out * scale).astype(jnp.bfloat16))
        return made

    sync = 1 + has_right.astype(jnp.int32) + has_left.astype(jnp.int32)
    sync += 2 + crossed.astype(jnp.int32) if square else n_sp - 1
    if DIRECT[0] and half > 2:
        sync += (z == half - 1).astype(jnp.int32)
        if ENDS[0] == 1:
            sync += (z == 0).astype(jnp.int32)
    pl.semaphore_wait(barrier, sync)
    loaded(0, xg_a.at[own, pl.ds(GAIN_ROWS, tokens)])
    x_start(0, 0)
    spread = [min(at, counts[0]) for at in PACE]
    for c in range(spread[0], spread[1]):
        x_start(0, c)
    loaded(1, w_a.at[mine])
    w_start(0)
    loaded(4, tables_buf)
    build_bias(tables_buf.at[0], rows_buf, tiles_a)
    for c in range(spread[1], spread[2]):
        x_start(0, c)
    build_bias(tables_buf.at[1], rows_buf, tiles_b)
    for c in range(spread[2], counts[0]):
        x_start(0, c)
    loaded(2, w_b.at[mine])

    last = half - 1

    def lead_end(layer):
        if layer == 0:
            for c in range(counts[0]):
                x_take(layer, c, 1)
            w_relay(0)
            w_start(1, (0,))

    def end_take(layer, c):
        for k in range(2 - layer, last + 1):
            x_take(layer, c, k)

    def lead_middle(layer):
        straight = min(DIRECT[layer], counts[layer])
        late = [2] if SWAP[layer] and last == 3 else []
        for c in range(straight):
            for k in range(1, last + 1):
                if k not in late:
                    x_take(layer, c, k)
        for k in range(1, last + 1, 2):
            for c in range(straight, counts[layer]):
                for one in range(k, min(k + 2, last + 1)):
                    x_take(layer, c, one)
            if k == 1 and layer == 0:
                w_relay(0)
        for c in range(straight):
            for k in late:
                x_take(layer, c, k)
        if layer == 0 and W_EARLY == 0:
            w_start(1, (0,))

    def handle(layer, rows):
        for at in range(0, len(rows), BATCH):
            batch = rows[at : at + BATCH]
            for index, made in zip(batch, attend(layer, batch)):
                if layer == 1:
                    out_ref[index * GRID_W : (index + 1) * GRID_W, :] = made
                else:
                    xg_b[own, pl.ds(place(1, index), GRID_W), :] = made

    for layer in range(2):
        pl.when(is_end)(functools.partial(lead_end, layer))
        if half > 2:
            pl.when(jnp.logical_not(is_end))(functools.partial(lead_middle, layer))
        chunks = counts[layer]
        taken = [0, 0]
        for c in range(chunks):
            for side in range(2):
                stop = min(AHEAD[layer][side][min(c, 3)], chunks) if chunks == 4 else c + 1
                for ask in range(taken[side], stop):
                    mine_now = is_end & (core == side)
                    pl.when(mine_now)(functools.partial(end_take, layer, ask))
                taken[side] = max(taken[side], stop)
            x_finish(layer, c)
            norm(layer, c)
            if c == 0:
                w_all(layer, 2 if square else n_sp - 1).wait_recv()
                if layer == 0 and square:
                    w_start(1, (1, 3))
            project(layer, c)

        if layer == 1 and rows_dev >= WIN_R:
            (_, middle), (up, above), (down, under) = row_groups(rows_dev, layer)
            low_first = sp <= n_sp // 4

            def finish_low():
                handle(layer, under + middle)

            def finish_high():
                handle(layer, middle)

            ask_down = functools.partial(halo_wait, layer, 0, [row for _, row in down])

            def low_side():
                ask_down()
                finish_low()

            def high_side():
                ask_down()
                handle(layer, under)

            pl.when(low_first)(low_side)
            pl.when(jnp.logical_not(low_first))(finish_high)
            halo_wait(layer, 1, [row for _, row in up])
            handle(layer, above)
            pl.when(jnp.logical_not(low_first))(high_side)
            continue

        finished, sent = set(), 0
        groups = row_groups(rows_dev, layer)
        for step, (waits, rows) in enumerate(groups):
            if layer == 0 and step == W_EARLY - 1 and half > 2:
                pl.when(jnp.logical_not(is_end))(functools.partial(w_start, 1, (0,)))
            if layer == 0 and step == min(W_STEP, len(groups) - 1):
                if square:
                    w_start(1, (2,))
                w_relay(1)
            for way in range(2):
                asked = [row for each, row in waits if each == way]
                if asked:
                    halo_wait(layer, way, asked)
            handle(layer, rows)
            finished |= set(rows)
            while layer == 0 and sent < counts[1]:
                if not set(orders[1][sent]) <= finished:
                    break
                x_start(1, sent)
                sent += 1

    for layer in range(2):
        for way in range(2):
            halo_sent(layer, way)
        w_all(layer, n_sp - 1).wait_send()
        x_drain(layer)


def body(n_sp, n_tp, stream, gain_a, wq_a, wk_a, wv_a, table_a, gain_b, wq_b, wk_b, wv_b, table_b):
    tokens, feat = stream.shape
    depth = wq_a.shape[0] * n_sp
    rows_dev = tokens // GRID_W
    chunks = max(len(order) for order in row_orders(rows_dev))
    bf16 = jnp.bfloat16
    padded = tokens + 2 * HALO * GRID_W
    hbm = pl.BlockSpec(memory_space=pl.ANY)
    vmem = pl.BlockSpec(memory_space=pltpu.VMEM)
    dma = pltpu.SemaphoreType.DMA
    return pl.pallas_call(
        functools.partial(kernel, n_sp, n_tp),
        out_shape=pltpu.VMEM((tokens, feat), bf16),
        in_specs=[hbm] * 11,
        out_specs=vmem,
        scratch_shapes=[
            pltpu.VMEM((n_tp, tokens + GAIN_ROWS, feat), bf16),
            pltpu.VMEM((n_tp, tokens, feat), bf16),
            pltpu.VMEM((depth, 3 * feat), bf16),
            pltpu.VMEM((depth, 3 * feat), bf16),
            pltpu.VMEM((padded, 2 * feat), bf16),
            pltpu.VMEM((padded, 2 * feat), bf16),
            pltpu.VMEM((tokens, feat), bf16),
            pltpu.VMEM((tokens, n_tp * feat), bf16),
            pltpu.VMEM((2, 1, feat), bf16),
            pltpu.VMEM((2, 2 * WIN_R - 1, 1, 2 * WIN_C - 1), jnp.float32),
            pltpu.VMEM((2 * WIN_R, 2 * GRID_W), jnp.float32),
            pltpu.VMEM((2 * WIN_R - 2, GRID_W, 2 * GRID_W), jnp.float32),
            pltpu.VMEM((2 * WIN_R - 2, GRID_W, 2 * GRID_W), jnp.float32),
            dma((5,)),
            dma,
            dma((2, chunks, n_tp // 2 - 1)),
            dma((2, chunks)),
            dma((2, 3)),
            dma((2 * HALO + 2,)),
        ],
        compiler_params=pltpu.CompilerParams(collective_id=0, has_side_effects=True),
    )(
        stream,
        gain_a.reshape(1, feat),
        gain_b.reshape(1, feat),
        wq_a,
        wk_a,
        wv_a,
        wq_b,
        wk_b,
        wv_b,
        jnp.transpose(table_a, (1, 0, 2)),
        jnp.transpose(table_b, (1, 0, 2)),
    )


def solution(mesh):
    placed = (
        P("sp", "tp"),
        P("tp"),
        P("sp", "tp"),
        P("sp", "tp"),
        P("sp", "tp"),
        P("tp", None, None),
        P("tp"),
        P("sp", "tp"),
        P("sp", "tp"),
        P("sp", "tp"),
        P("tp", None, None),
    )
    return jax.shard_map(
        functools.partial(body, mesh.shape["sp"], mesh.shape["tp"]),
        mesh=mesh,
        in_specs=placed,
        out_specs=P("sp", "tp"),
        check_vma=False,
    )
```
